32 devices in a mesh: sp: 8 (over z, x), dp: 4 (over y, core).
Axes of the slice: x: 2, y: 2, z: 4, core: 2. Of those that a mesh axis runs over, the one named last changes fastest.
Arguments:
- resid: bfloat16 [4, 1024, 2048], P('dp', 'sp'), may hold values from -6 to 6
- queries: bfloat16 [4, 1024, 2048], P('dp', 'sp'), may hold values from -7 to 7
- keys: bfloat16 [4, 1024, 2048], P('dp', 'sp'), may hold values from -7 to 7
- values: bfloat16 [4, 1024, 2048], P('dp', 'sp'), may hold values from -6 to 6
- forget_cache: float32 [4, 32, 1024], P('dp', 'sp'), may hold values from -131 to 0, as said below
- query_gain: float32 [64], replicated, may hold values from 0.5 to 8
- key_gain: float32 [64], replicated, may hold values from 0.5 to 8
- out_weight: bfloat16 [2048, 2048], P(None, 'dp'), may hold values from -0.125 to 0.125
- norm_gain: float32 [2048], replicated, may hold values from 0.1 to 1.9
- routes: int32 [4, 1024, 2], P('dp', 'sp'), may hold values from 0 to 31, all different within a row; in each aligned block of 128 rows (0 to 127, 128 to 255, ..., all dimensions but the last counted through in order) at most 16 rows name the same one
- group_weight: float32 [4, 1024], P('dp', 'sp'), may hold values from 0.2 to 1
- inner_share: float32 [4, 1024, 2], P('dp', 'sp'), may hold values from 0.1 to 1
- expert_gate: bfloat16 [32, 2048, 1024], P(('sp', 'dp')), may hold values from -0.125 to 0.125
- expert_up: bfloat16 [32, 2048, 1024], P(('sp', 'dp')), may hold values from -0.125 to 0.125
- expert_down: bfloat16 [32, 1024, 2048], P(('sp', 'dp')), may hold values from -0.1875 to 0.1875
Outputs:
- layer_out: bfloat16 [4, 1024, 2048], P('dp', 'sp')
The draws below stay inside these ranges and needn't reach their ends.
Inputs may be any that keep to these rules, and one draw needn't show every extreme that they name: `routes`: each row names 2 different experts; the rows of one device name one expert at most 16 times, a bound that some block reaches. `forget_cache`: along positions each head's values never rise.
All inputs are finite; a program needn't handle non-finite values.
Results may differ from the reference program's by a relative error of at most 0.0095.
The reference program's roundings to bfloat16 on the way count: a program that leaves them out, or rounds other values in their place, can miss the bound.
Values may be sent and summed in bfloat16 or wider, within the bound.
A program may use at most 128 MiB of HBM per device.

```python
import math
import jax
import jax.numpy as jnp
import numpy as np
from jax import lax

D = 2048
HEAD_COUNT = 32
HD = 64
FF = 1024
TOPK = 2
TOK_DEV = 128
SEQUENCE_COUNT = 4
SEQUENCE_LENGTH = 1024
EXPERTS = 32
CAP = 16


def paired_rows(key):
    base = jax.random.fold_in(key, 7)
    key_q, key_k = jax.random.split(base, 2)
    shape = (SEQUENCE_COUNT, SEQUENCE_LENGTH, HEAD_COUNT * HD)
    key_rows = jax.random.truncated_normal(key_k, -6.0, 6.0, shape, jnp.float32)
    query_rows = jax.random.truncated_normal(key_q, -6.0, 6.0, shape, jnp.float32)
    return (query_rows, key_rows)


def draw_queries(key, part):
    return paired_rows(key)[0].astype(jnp.bfloat16)


def draw_keys(key, part):
    return paired_rows(key)[1].astype(jnp.bfloat16)


def draw_query_gain(key, part):
    sub = jax.random.fold_in(key, 11)
    return jax.random.uniform(sub, (HD,), jnp.float32, 0.5, 1.5)


def draw_key_gain(key, part):
    sub = jax.random.fold_in(key, 13)
    return jax.random.uniform(sub, (HD,), jnp.float32, 0.5, 1.5)


def draw_forget_cache(key, part):
    random_keys = jax.random.split(jax.random.fold_in(key, 17), 7)
    order = jax.random.permutation(random_keys[0], HEAD_COUNT)
    slow = order < HEAD_COUNT // 2
    total = jax.random.uniform(random_keys[1], (SEQUENCE_COUNT, HEAD_COUNT), jnp.float32, 0.3, 1.0)
    fast_span = jax.random.uniform(random_keys[2], (SEQUENCE_COUNT, HEAD_COUNT), jnp.float32, 30.0, 100.0)
    rate = jnp.where(slow[None, :], total / SEQUENCE_LENGTH, 1.0 / fast_span)
    blocks = SEQUENCE_LENGTH // TOK_DEV
    factor = jnp.exp(jax.random.uniform(random_keys[3], (SEQUENCE_COUNT, HEAD_COUNT, blocks), jnp.float32, -0.693, 0.693))
    factor = jnp.repeat(factor, TOK_DEV, axis=2)
    rough = jax.random.uniform(random_keys[4], (SEQUENCE_COUNT, HEAD_COUNT, SEQUENCE_LENGTH), jnp.float32, 0.3, 1.7)
    baseline_level = -rate[:, :, None] * factor * rough
    spike_location = jax.random.randint(random_keys[5], (SEQUENCE_COUNT, HEAD_COUNT, 3), 0, SEQUENCE_LENGTH)
    spike_dropped = jnp.log(jax.random.uniform(random_keys[6], (SEQUENCE_COUNT, HEAD_COUNT, 3), jnp.float32, 0.5, 0.8))
    token_offset = jnp.arange(SEQUENCE_LENGTH, dtype=jnp.int32)
    spike_events = jnp.sum(jnp.where(token_offset[None, None, None, :] == spike_location[..., None], spike_dropped[..., None], 0.0), axis=2)
    return jnp.cumsum(baseline_level + spike_events, axis=2)


def level_of(own_key, dims, cuts, smallest, top_value):
    def one(dim, parts):
        heights = jax.random.uniform(jax.random.fold_in(jax.random.fold_in(own_key, 6), dim), (parts,), jnp.float32, smallest / len(cuts), top_value / len(cuts))
        return jnp.repeat(jnp.exp(heights), dims[dim] // parts).reshape((-1,) + (1,) * (len(dims) - dim - 1))

    level = one(*cuts[0])
    for cut in cuts[1:]:
        level = level * one(*cut)
    return level


def shared_out(key, own, number, rows, count, top, bound, lean):
    ranking = jax.random.permutation(key, count)
    packed, ordinary = portions_of(count, rows * top, bound, lean, True), portions_of(count, rows * top, bound, lean, False)
    places = jnp.arange(count)

    def named(tallies, offset_by):
        used = int((tallies > 0).sum())
        fixed = max(1, used // 4)
        moved = fixed + (places - fixed + offset_by * (used - fixed)) % max(1, count - fixed)
        return jnp.zeros((count,), jnp.int32).at[ranking[jnp.where(places < fixed, places, moved)]].set(jnp.asarray(tallies, jnp.int32))

    tallies = jnp.where(number % 4 == 0, named(packed, number // 4), named(ordinary, number - number // 4 - 1))
    mixed = jax.random.permutation(jax.random.fold_in(own, 3), count)
    source_of, receiver = mixed[0:count // 2 * 2:2], mixed[1:count // 2 * 2:2]
    margin = jnp.minimum(tallies[source_of] - 1, bound - tallies[receiver]) // 2
    margin = jnp.where((source_of == ranking[0]) | (receiver == ranking[0]) | (tallies[receiver] == 0), 0, jnp.maximum(margin, 0))
    moved = jax.random.randint(jax.random.fold_in(own, 4), (count // 2,), 0, 1 << 20) % (margin + 1)
    tallies = tallies.at[source_of].add(-moved).at[receiver].add(moved)
    members = jnp.searchsorted(jnp.cumsum(tallies), jnp.arange(rows * top), side="right").astype(jnp.int32)
    listing = members.reshape(top, rows).T
    listing = listing[jax.random.permutation(jax.random.fold_in(own, 1), rows)]
    offset_by = jax.random.randint(jax.random.fold_in(own, 2), (rows, 1), 0, top)
    return jnp.take_along_axis(listing, (jnp.arange(top)[None, :] + offset_by) % top, axis=1)


def portions_of(number_of, total, limit, lean, full):
    loads = [(1 << 20) // math.isqrt(grade ** lean) + 1 for grade in range(1, number_of + 1)]
    largest = limit if full else min(limit, max(-(-total // number_of), total * loads[0] // sum(loads)))
    least = 1 if total - largest >= number_of - 1 else 0
    counts, surplus = [largest] + [least] * (number_of - 1), total - largest - least * (number_of - 1)
    while surplus > 0:
        free = [i for i in range(1, number_of) if counts[i] < largest] or [i for i in range(1, number_of) if counts[i] < limit]
        pool, remaining = sum([loads[i] for i in free]), surplus
        for i in free:
            extra = min(limit - counts[i], max(1, remaining * loads[i] // pool), surplus)
            counts[i] = counts[i] + extra
            surplus = surplus - extra
    return np.array(counts)


def centred(key, dims, width, limit, shards=(), kind=jnp.bfloat16):
    entries = jax.random.normal(key, dims, jnp.float32) * width
    if len(shards) > 0:
        entries = level_of(key, dims, shards, -0.22, 0.18) * entries
    return jnp.clip(entries, min=-limit, max=limit).astype(kind)


def setup_inputs(seed: int = 0) -> dict:
    key_of = jax.random.split(jax.random.key(seed), 16)
    resid = centred(key_of[0], (SEQUENCE_COUNT, SEQUENCE_LENGTH, D), 1.0, 6.0, ((0, 4), (1, 8)))
    queries = draw_queries(jax.random.fold_in(key_of[15], 71), 0)
    keys = draw_keys(jax.random.fold_in(key_of[15], 71), 0)
    values = centred(key_of[3], (SEQUENCE_COUNT, SEQUENCE_LENGTH, HEAD_COUNT * HD), 1.0, 6.0, ((0, 4), (1, 8)))
    forget_cache = draw_forget_cache(jax.random.fold_in(key_of[15], 71), 0)
    query_gain = draw_query_gain(jax.random.fold_in(key_of[15], 71), 0)
    key_gain = draw_key_gain(jax.random.fold_in(key_of[15], 71), 0)
    out_weight = centred(key_of[7], (HEAD_COUNT * HD, D), (HEAD_COUNT * HD) ** -0.5, 0.125, ((1, 4),))
    norm_gain = jnp.clip(1.0 + 0.18 * jax.random.normal(key_of[8], (D,), jnp.float32), 0.1, 1.9)
    routes_keys = jax.random.split(jax.random.fold_in(key_of[9], 1), SEQUENCE_COUNT * SEQUENCE_LENGTH // TOK_DEV)
    routes_turns = jax.random.permutation(jax.random.fold_in(key_of[9], 3), SEQUENCE_COUNT * SEQUENCE_LENGTH // TOK_DEV)
    routes = jax.vmap(lambda own, number: shared_out(jax.random.fold_in(key_of[9], 2), own, number, TOK_DEV, EXPERTS, TOPK, CAP, 2))(routes_keys, routes_turns).reshape((SEQUENCE_COUNT, SEQUENCE_LENGTH, TOPK))
    group_weight = jnp.clip(jnp.exp(math.log(1.0) - 1.609438 * jax.random.uniform(key_of[10], (SEQUENCE_COUNT, SEQUENCE_LENGTH), jnp.float32) ** level_of(key_of[10], (SEQUENCE_COUNT, SEQUENCE_LENGTH), ((0, 4), (1, 8)), -0.2, 0.2)), 0.2, 1.0)
    inner_share = jnp.clip(jnp.exp(math.log(1.0) - 2.3025851 * jax.random.uniform(key_of[11], (SEQUENCE_COUNT, SEQUENCE_LENGTH, TOPK), jnp.float32) ** level_of(key_of[11], (SEQUENCE_COUNT, SEQUENCE_LENGTH, TOPK), ((0, 4), (1, 8)), -0.2, 0.2)), 0.1, 1.0)
    expert_gate = centred(key_of[12], (EXPERTS, D, FF), D ** -0.5, 0.125, ((0, 32),))
    expert_up = centred(key_of[13], (EXPERTS, D, FF), D ** -0.5, 0.125, ((0, 32),))
    expert_down = centred(key_of[14], (EXPERTS, FF, D), FF ** -0.5, 0.1875, ((0, 32),))
    return dict(resid=resid, queries=queries, keys=keys, values=values, forget_cache=forget_cache, query_gain=query_gain, key_gain=key_gain, out_weight=out_weight, norm_gain=norm_gain, routes=routes, group_weight=group_weight, inner_share=inner_share, expert_gate=expert_gate, expert_up=expert_up, expert_down=expert_down)


EPS = 1e-06

def norm_rows(inputs, gain):
    floats = inputs.astype(jnp.float32)
    scaled = floats * lax.rsqrt(lax.optimization_barrier(jnp.mean(floats * floats, axis=-1, keepdims=True)) + EPS)
    return (scaled * gain.astype(jnp.float32)).astype(jnp.bfloat16)

def head_attention(operands):
    query_rows, key_rows, value_rows, decay = operands
    scores = jnp.dot(query_rows, key_rows.T, preferred_element_type=jnp.float32) * HD ** (-0.5)
    scores = scores + decay[:, None] - decay[None, :]
    token_offset = jnp.arange(query_rows.shape[0], dtype=jnp.int32)
    scores = jnp.where(token_offset[None, :] <= token_offset[:, None], scores, -jnp.inf)
    highest = lax.optimization_barrier(jnp.max(scores, axis=-1, keepdims=True))
    expd = jnp.exp(scores - highest)
    probs = (expd / lax.optimization_barrier(jnp.sum(expd, axis=-1, keepdims=True))).astype(jnp.bfloat16)
    return jnp.dot(probs, value_rows, preferred_element_type=jnp.float32).astype(jnp.bfloat16)

def reference(resid, queries, keys, values, forget_cache, query_gain, key_gain, out_weight, norm_gain, routes, group_weight, inner_share, expert_gate, expert_up, expert_down):

    def sequence_attention(operands):
        seq_q, seq_k, seq_v, seq_c = operands
        query_normed = norm_rows(seq_q.reshape(SEQUENCE_LENGTH, HEAD_COUNT, HD), query_gain).transpose(1, 0, 2)
        key_normed = norm_rows(seq_k.reshape(SEQUENCE_LENGTH, HEAD_COUNT, HD), key_gain).transpose(1, 0, 2)
        value_heads = seq_v.reshape(SEQUENCE_LENGTH, HEAD_COUNT, HD).transpose(1, 0, 2)
        outputs = lax.map(head_attention, (query_normed, key_normed, value_heads, seq_c))
        return outputs.transpose(1, 0, 2).reshape(SEQUENCE_LENGTH, HEAD_COUNT * HD)
    attn = lax.map(sequence_attention, (queries, keys, values, forget_cache))
    projected = jnp.dot(attn.reshape(-1, HEAD_COUNT * HD), out_weight, preferred_element_type=jnp.float32)
    mid = (resid.reshape(-1, D).astype(jnp.float32) + projected).astype(jnp.bfloat16)
    normed = norm_rows(mid, norm_gain)
    shares = inner_share.reshape(-1, TOPK).astype(jnp.float32)
    weights = group_weight.reshape(-1, 1).astype(jnp.float32) * shares / lax.optimization_barrier(jnp.sum(shares, axis=-1, keepdims=True))
    flat_weights = weights.reshape(-1)
    flat_routes = routes.reshape(-1).astype(jnp.int32)
    slot_count = EXPERTS * CAP
    slot_place = jnp.arange(slot_count, dtype=jnp.int32)

    def one_expert(total, expert_index):
        hit = flat_routes == expert_index
        hit_count = jnp.sum(hit.astype(jnp.int32))
        picked = jnp.nonzero(hit, size=slot_count, fill_value=0)[0].astype(jnp.int32)
        live = slot_place < hit_count
        token_index = (picked // TOPK).astype(jnp.int32)
        rows = normed[token_index]
        gate = jnp.dot(rows, expert_gate[expert_index], preferred_element_type=jnp.float32)
        upper = jnp.dot(rows, expert_up[expert_index], preferred_element_type=jnp.float32)
        hidden = (jax.nn.silu(gate) * upper).astype(jnp.bfloat16)
        result = jnp.dot(hidden, expert_down[expert_index], preferred_element_type=jnp.float32).astype(jnp.bfloat16)
        scale = jnp.where(live, flat_weights[picked], jnp.zeros_like(flat_weights[picked]))
        total = total.at[token_index].add(result.astype(jnp.float32) * scale[:, None])
        return (total, None)
    start = jnp.zeros((mid.shape[0], D), jnp.float32)
    mixed, _ = lax.scan(one_expert, start, jnp.arange(EXPERTS, dtype=jnp.int32))
    layer_out = (mid.astype(jnp.float32) + mixed).astype(jnp.bfloat16)
    return layer_out.reshape(SEQUENCE_COUNT, SEQUENCE_LENGTH, D)
```

```python
import functools

import jax
import jax.numpy as jnp
from jax import lax
from jax.experimental import pallas as pl
from jax.experimental.pallas import tpu as pltpu
from jax.sharding import PartitionSpec as P

EPS = 1e-06


MESH = pl.DeviceIdType.MESH
LANES = 128
BLOCK = 256


def place(index, size):
    return pl.ds(pl.multiple_of(index * size, size), size)


def half_means(squares, head_size):
    lane = lax.broadcasted_iota(jnp.int32, (LANES, LANES), 0) // head_size
    other = lax.broadcasted_iota(jnp.int32, (LANES, LANES), 1) // head_size
    same = (lane == other).astype(jnp.float32).astype(jnp.bfloat16)
    high = squares.astype(jnp.bfloat16)
    low = (squares - high.astype(jnp.float32)).astype(jnp.bfloat16)
    total = jnp.dot(high, same, preferred_element_type=jnp.float32)
    total = total + jnp.dot(low, same, preferred_element_type=jnp.float32)
    return total * (1.0 / head_size)


def attention_stage(
    n, dp_size, head_size, small_loads, weight_loads,
    q_ref, k_ref, v_ref, weight_ref, resid_ref,
    decay_ref, q_gain_ref, k_gain_ref, norm_gain_ref, routes_ref, group_ref, share_ref,
    mid_ref, normed_ref, info_ref, out_ref, weights, resid_buf,
    q_buf, k_buf, v_buf, q_norm, k_head, v_ones, o_buf,
    local_sem, send_sem, recv_sem, own_sem, back_send, back_recv,
    weight_sem, weight_send, weight_recv, pass_send, pass_recv, resid_sem,
):
    me = lax.axis_index("sp")
    column = lax.axis_index("dp")
    rows_y = dp_size // 2
    row_y, core = column // 2, column % 2
    twin = row_y * 2 + 1 - core
    tok = q_ref.shape[0]
    pairs, length = q_buf.shape[0], q_buf.shape[1]
    inner = LANES // head_size
    sources, buffers = (q_ref, k_ref, v_ref), (q_buf, k_buf, v_buf)

    def weight_across(step):
        return pltpu.make_async_remote_copy(
            src_ref=weight_ref,
            dst_ref=weights.at[column],
            send_sem=weight_send.at[step],
            recv_sem=weight_recv.at[step],
            device_id={"dp": lax.rem(row_y + step, rows_y) * 2 + core},
            device_id_type=MESH,
        )

    def weight_pass(step):
        block = lax.rem(row_y + rows_y - step, rows_y) * 2 + core
        return pltpu.make_async_remote_copy(
            src_ref=weight_ref if step == 0 else weights.at[block],
            dst_ref=weights.at[block],
            send_sem=pass_send.at[step],
            recv_sem=pass_recv.at[step],
            device_id={"dp": twin},
            device_id_type=MESH,
        )

    weight_own = pltpu.make_async_copy(weight_ref, weights.at[column], weight_sem)

    def outgoing(kind, pair, step):
        target = lax.rem(me + step, n)
        return pltpu.make_async_remote_copy(
            src_ref=sources[kind].at[:, place(target * pairs + pair, LANES)],
            dst_ref=buffers[kind].at[pair, place(me, tok), :],
            send_sem=send_sem.at[kind, pair, step],
            recv_sem=recv_sem.at[kind, pair, step],
            device_id={"sp": target},
            device_id_type=MESH,
        )

    def own(kind, pair):
        return pltpu.make_async_copy(
            sources[kind].at[:, place(me * pairs + pair, LANES)],
            buffers[kind].at[pair, place(me, tok), :],
            local_sem.at[kind, pair],
        )

    def backward(pair, step):
        target = lax.rem(me + step, n)
        return pltpu.make_async_remote_copy(
            src_ref=o_buf.at[pair, place(target, tok), :],
            dst_ref=out_ref.at[:, place(me * pairs + pair, LANES)],
            send_sem=back_send.at[pair, step],
            recv_sem=back_recv.at[pair, step],
            device_id={"sp": target},
            device_id_type=MESH,
        )

    def own_back(pair):
        return pltpu.make_async_copy(
            o_buf.at[pair, place(me, tok), :],
            out_ref.at[:, place(me * pairs + pair, LANES)],
            own_sem.at[pair],
        )

    for pair in range(pairs):
        for step in range(1, n):
            for kind in range(3):
                outgoing(kind, pair, step).start()
        for kind in range(3):
            own(kind, pair).start()

    for step in range(1, rows_y):
        weight_across(step).start()
    weight_pass(0).start()
    weight_own.start()
    load_resid = pltpu.make_async_copy(resid_ref, resid_buf, resid_sem)
    load_resid.start()
    for load in weight_loads:
        load.start()
    for load in small_loads:
        load.wait()
    info_ref[...] = routing_info(routes_ref, group_ref, share_ref, n * dp_size)
    q_gain = jnp.concatenate([q_gain_ref[...]] * inner, axis=1)
    k_gain = jnp.concatenate([k_gain_ref[...]] * inner, axis=1)

    row = lax.broadcasted_iota(jnp.int32, (BLOCK, BLOCK), 0)
    col = lax.broadcasted_iota(jnp.int32, (BLOCK, BLOCK), 1)
    lane = lax.broadcasted_iota(jnp.int32, (length, LANES), 1) // head_size
    out_lane = lax.broadcasted_iota(jnp.int32, (BLOCK, LANES), 1) // head_size
    scale = head_size ** (-0.5)
    v_ones[:, LANES:] = jnp.ones((length, LANES), jnp.bfloat16)

    def scores_of(queries, keys):
        return lax.dot_general(
            queries, keys, (((1,), (1,)), ((), ())), preferred_element_type=jnp.float32
        )

    def one_pair(pair, carry):
        for kind in range(3):
            own(kind, pair).wait()
            for step in range(1, n):
                outgoing(kind, pair, step).wait_recv()
        floats = q_buf[pair].astype(jnp.float32)
        floats = floats * lax.rsqrt(half_means(floats * floats, head_size) + EPS)
        normed = (floats * q_gain).astype(jnp.bfloat16)
        q_norm[...] = (normed.astype(jnp.float32) * scale).astype(jnp.bfloat16)
        floats = k_buf[pair].astype(jnp.float32)
        floats = floats * lax.rsqrt(half_means(floats * floats, head_size) + EPS)
        floats = floats * k_gain
        for head in range(inner):
            k_head[head] = jnp.where(lane == head, floats, 0.0).astype(jnp.bfloat16)
        v_ones[:, :LANES] = v_buf[pair]
        for block in range(length // BLOCK):
            first = block * BLOCK
            here = slice(first, first + BLOCK)
            query_block = q_norm[here, :]
            merged = None
            for head in range(inner):
                decay = decay_ref[pl.ds(pair * inner + head, 1), :]
                decay_here = decay[:, here]
                query_decay = jnp.sum(
                    jnp.where(row == col, decay_here, 0.0), axis=1, keepdims=True
                )
                near = scores_of(query_block, k_head[head, here, :])
                near = near + (query_decay - decay_here)
                near = jnp.where(col <= row, near, -jnp.inf)
                highest = jnp.max(near, axis=1, keepdims=True)
                if block > 0:
                    far = scores_of(query_block, k_head[head, :first, :])
                    far = far + (query_decay - decay[:, :first])
                    highest = jnp.maximum(highest, jnp.max(far, axis=1, keepdims=True))
                total = jnp.dot(
                    jnp.exp(near - highest).astype(jnp.bfloat16),
                    v_ones[here, :],
                    preferred_element_type=jnp.float32,
                )
                if block > 0:
                    total = total + jnp.dot(
                        jnp.exp(far - highest).astype(jnp.bfloat16),
                        v_ones[:first, :],
                        preferred_element_type=jnp.float32,
                    )
                result = total[:, :LANES] / total[:, LANES:]
                merged = result if head == 0 else jnp.where(out_lane == head, result, merged)
            o_buf[pair, here, :] = merged.astype(jnp.bfloat16)
        for step in range(1, n):
            backward(pair, step).start()
        own_back(pair).start()
        return carry

    lax.fori_loop(0, pairs, one_pair, 0)
    for step in range(1, rows_y):
        weight_across(step).wait_recv()
        weight_pass(step).start()

    def finish(pair, carry):
        own_back(pair).wait()
        for step in range(1, n):
            backward(pair, step).wait()
            for kind in range(3):
                outgoing(kind, pair, step).wait_send()
        return carry

    lax.fori_loop(0, pairs, finish, 0)
    weight_own.wait()
    for step in range(1, rows_y):
        weight_across(step).wait_send()
    for step in range(rows_y):
        weight_pass(step).wait()
    load_resid.wait()
    span = weights.shape[2]
    squares = jnp.zeros((tok, 1), jnp.float32)
    for block in range(dp_size):
        columns = slice(block * span, (block + 1) * span)
        projected = jnp.dot(
            out_ref[...], weights[block], preferred_element_type=jnp.float32
        )
        mid = (resid_buf[:, columns].astype(jnp.float32) + projected).astype(jnp.bfloat16)
        mid_ref[:, columns] = mid
        floats = mid.astype(jnp.float32)
        squares = squares + jnp.sum(floats * floats, axis=1, keepdims=True)
    factor = lax.rsqrt(squares * (1.0 / (dp_size * span)) + EPS)
    for block in range(dp_size):
        columns = slice(block * span, (block + 1) * span)
        scaled = mid_ref[:, columns].astype(jnp.float32) * factor
        normed_ref[:, columns] = (scaled * norm_gain_ref[:, columns]).astype(jnp.bfloat16)


INFO_ROWS = 8


def routing_info(routes_ref, group_ref, share_ref, experts):
    top, tok = routes_ref.shape
    capacity = 2 * tok * top // experts
    expert = lax.broadcasted_iota(jnp.int32, (experts, tok), 0)
    hits = [(expert == routes_ref[r : r + 1, :]).astype(jnp.float32) for r in range(top)]
    every = sum(hits[1:], hits[0]).astype(jnp.bfloat16)
    row = lax.broadcasted_iota(jnp.int32, (tok, tok), 0)
    col = lax.broadcasted_iota(jnp.int32, (tok, tok), 1)
    before = (row < col).astype(jnp.float32).astype(jnp.bfloat16)
    earlier = jnp.dot(every, before, preferred_element_type=jnp.float32)
    shares = [share_ref[r : r + 1, :] for r in range(top)]
    total = sum(shares[1:], shares[0])
    lines = [
        routes_ref[r : r + 1, :].astype(jnp.float32) * capacity
        + jnp.sum(hits[r] * earlier, axis=0, keepdims=True)
        for r in range(top)
    ]
    lines += [group_ref[...] * shares[r] / total for r in range(top)]
    lines.append(jnp.zeros((INFO_ROWS - 2 * top, tok), jnp.float32))
    return jnp.concatenate(lines, axis=0)


CHUNKS = 4


def expert_stage(
    sp_size, dp_size, per, top, weight_loads,
    mid_ref, normed_ref, info_ref, gate_buf, up_buf, down_buf,
    out_ref,
    far_rows, far_info, packed, arrived, result, returned, partial, incoming,
    info_sem, row_send, row_recv, send_sem, recv_sem,
    back_send, back_recv, sum_send, sum_recv,
):
    n = sp_size * dp_size
    half = n // 2
    me = lax.axis_index("sp") * dp_size + lax.axis_index("dp")
    side, seat = me // half, me % half
    twin = (me + half) % n
    tok, width = normed_ref.shape
    cap = packed.shape[2]
    part = width // CHUNKS
    mine = half // 2

    def columns(chunk):
        return slice(chunk * part, (chunk + 1) * part)

    def coords(flat):
        return {"sp": flat // dp_size, "dp": flat % dp_size}

    info_copy = pltpu.make_async_remote_copy(
        src_ref=info_ref, dst_ref=far_info, send_sem=info_sem.at[0], recv_sem=info_sem.at[1],
        device_id=coords(twin), device_id_type=MESH,
    )
    row_copies = [
        pltpu.make_async_remote_copy(
            src_ref=normed_ref.at[:, columns(chunk)],
            dst_ref=far_rows.at[:, columns(chunk)],
            send_sem=row_send.at[chunk],
            recv_sem=row_recv.at[chunk],
            device_id=coords(twin),
            device_id_type=MESH,
        )
        for chunk in range(CHUNKS)
    ]

    def outgoing(kind, step, chunk):
        target = (seat + mine + step) % half
        return pltpu.make_async_remote_copy(
            src_ref=packed.at[kind, target, :, columns(chunk)],
            dst_ref=arrived.at[kind, step, :, columns(chunk)],
            send_sem=send_sem.at[kind, chunk, step],
            recv_sem=recv_sem.at[kind, chunk, step],
            device_id=coords(side * half + target),
            device_id_type=MESH,
        )

    def backward(kind, step, chunk):
        target = (seat + half + half - mine - step) % half
        return pltpu.make_async_remote_copy(
            src_ref=result.at[kind, step, :, columns(chunk)],
            dst_ref=returned.at[kind, seat, :, columns(chunk)],
            send_sem=back_send.at[kind, chunk, step],
            recv_sem=back_recv.at[kind, chunk, step],
            device_id=coords(side * half + target),
            device_id_type=MESH,
        )

    def sum_copy(chunk):
        return pltpu.make_async_remote_copy(
            src_ref=partial.at[chunk],
            dst_ref=incoming.at[chunk],
            send_sem=sum_send.at[chunk],
            recv_sem=sum_recv.at[chunk],
            device_id=coords(twin),
            device_id_type=MESH,
        )

    def others(action, start=0, stop=half):
        def run(step, carry):
            @pl.when(step != mine)
            def _():
                action(step)

            return carry

        lax.fori_loop(start, stop, run, 0)

    first_slot = (side * (half * cap)).astype(jnp.float32)

    def dispatch(kind, source_ref, route_ref, chunk):
        slot = lax.broadcasted_iota(jnp.int32, (half * cap, tok), 0).astype(jnp.float32)
        hit = jnp.zeros((half * cap, tok), jnp.float32)
        for route in range(top):
            local = route_ref[route : route + 1, :] - first_slot
            hit = hit + jnp.where(slot == local, 1.0, 0.0)
        rows = jnp.dot(
            hit.astype(jnp.bfloat16), source_ref[:, columns(chunk)],
            preferred_element_type=jnp.float32,
        )
        packed[kind, :, :, columns(chunk)] = rows.astype(jnp.bfloat16).reshape(half, cap, part)
        others(lambda step: outgoing(kind, step, chunk).start())
        arrived[kind, mine, :, columns(chunk)] = packed[kind, seat, :, columns(chunk)]

    def forward(kind, send_back):
        def group(index, carry):
            first = index * per

            def take(step):
                for chunk in range(CHUNKS):
                    outgoing(kind, step, chunk).wait_recv()

            others(take, first, first + per)
            rows = arrived[kind, pl.ds(first, per)].reshape(per * cap, width)
            gate = jnp.dot(rows, gate_buf[...], preferred_element_type=jnp.float32)
            upper = jnp.dot(rows, up_buf[...], preferred_element_type=jnp.float32)
            hidden = (gate / (1.0 + jnp.exp(-gate)) * upper).astype(jnp.bfloat16)
            for chunk in range(CHUNKS):
                product = jnp.dot(
                    hidden, down_buf[:, columns(chunk)], preferred_element_type=jnp.float32
                )
                result[kind, pl.ds(first, per), :, columns(chunk)] = product.astype(
                    jnp.bfloat16
                ).reshape(per, cap, part)
                if send_back:
                    others(lambda step: backward(kind, step, chunk).start(), first, first + per)
            return carry

        lax.fori_loop(0, half // per, group, 0)
        returned[kind, seat] = result[kind, mine]

    row = lax.broadcasted_iota(jnp.int32, (tok, tok), 0)
    col = lax.broadcasted_iota(jnp.int32, (tok, tok), 1)

    def upright(line):
        return jnp.sum(jnp.where(row == col, line, 0.0), axis=1, keepdims=True)

    def choices(route_ref):
        slot = lax.broadcasted_iota(jnp.int32, (tok, half * cap), 1).astype(jnp.float32)
        picks = []
        for route in range(top):
            local = upright(route_ref[route : route + 1, :]) - first_slot
            pick = jnp.where(slot == local, 1.0, 0.0).astype(jnp.bfloat16)
            picks.append((pick, upright(route_ref[top + route : top + route + 1, :])))
        return picks

    def combine(kind, picks, chunk):
        others(lambda step: backward(kind, step, chunk).wait_recv())
        block = returned[kind, :, :, columns(chunk)].reshape(half * cap, part)
        total = None
        for pick, weight in picks:
            term = weight * jnp.dot(pick, block, preferred_element_type=jnp.float32)
            total = term if total is None else total + term
        return total

    info_copy.start()
    for copy in row_copies:
        copy.start()
    for chunk in range(CHUNKS):
        dispatch(0, normed_ref, info_ref, chunk)
    info_copy.wait_recv()
    for chunk in range(CHUNKS):
        row_copies[chunk].wait_recv()
        dispatch(1, far_rows, far_info, chunk)
    for load in weight_loads:
        load.wait()
    forward(0, False)
    forward(1, True)
    for chunk in range(CHUNKS):
        others(lambda step: backward(0, step, chunk).start())
    far_picks = choices(far_info)
    for chunk in range(CHUNKS):
        partial[chunk] = combine(1, far_picks, chunk).astype(jnp.bfloat16)
        sum_copy(chunk).start()
    picks = choices(info_ref)
    for chunk in range(CHUNKS):
        total = combine(0, picks, chunk)
        sum_copy(chunk).wait_recv()
        total = total + incoming[chunk].astype(jnp.float32)
        out_ref[:, columns(chunk)] = mid_ref[:, columns(chunk)].astype(jnp.float32) + total

    info_copy.wait_send()
    for chunk in range(CHUNKS):
        row_copies[chunk].wait_send()
        sum_copy(chunk).wait_send()

    def drain(step):
        for kind in range(2):
            for chunk in range(CHUNKS):
                outgoing(kind, step, chunk).wait_send()
                backward(kind, step, chunk).wait_send()

    others(drain)


def layer_kernel(sp_size, dp_size, head_size, per, top, *refs):
    inputs, out_ref, scratch = refs[:15], refs[15], refs[16:]
    (
        q_ref, k_ref, v_ref, weight_ref, resid_ref, gate_ref, up_ref, down_ref,
    ) = inputs[:8]
    small = scratch[:7]
    gate_buf, up_buf, down_buf, mid_ref, normed_ref, info_ref = scratch[7:13]
    small_sem, load_sem = scratch[13:15]
    attention_scratch, expert_scratch = scratch[15:37], scratch[37:]
    small_loads = [
        pltpu.make_async_copy(source, target, small_sem.at[index])
        for index, (source, target) in enumerate(zip(inputs[8:], small))
    ]
    weight_loads = [
        pltpu.make_async_copy(source, target, load_sem.at[index])
        for index, (source, target) in enumerate(
            ((gate_ref, gate_buf), (up_ref, up_buf), (down_ref, down_buf))
        )
    ]
    for load in small_loads:
        load.start()
    n = sp_size * dp_size
    me = lax.axis_index("sp") * dp_size + lax.axis_index("dp")
    barrier = pltpu.get_barrier_semaphore()

    def greet(step, carry):
        other = (me + step) % n
        pl.semaphore_signal(
            barrier, inc=1, device_id={"sp": other // dp_size, "dp": other % dp_size},
            device_id_type=MESH,
        )
        return carry

    lax.fori_loop(1, n, greet, 0)
    pl.semaphore_wait(barrier, n - 1)
    attention_stage(
        sp_size, dp_size, head_size, small_loads, weight_loads,
        q_ref, k_ref, v_ref, weight_ref, resid_ref, *small,
        mid_ref, normed_ref, info_ref, *attention_scratch,
    )
    expert_stage(
        sp_size, dp_size, per, top, weight_loads,
        mid_ref, normed_ref, info_ref, gate_buf, up_buf, down_buf, out_ref, *expert_scratch,
    )


def run_layer(
    queries, keys, values, out_weight, resid, gate, upper, down,
    decay, query_gain, key_gain, norm_gain, routes, group_weight, inner_share,
):
    tok, width = queries.shape
    sp_size, dp_size = lax.axis_size("sp"), lax.axis_size("dp")
    top = routes.shape[0]
    head_size = query_gain.shape[1]
    inner = LANES // head_size
    pairs = width // sp_size // LANES
    length = sp_size * tok
    n = sp_size * dp_size
    half = n // 2
    cap = 2 * tok * top // n
    per = max(1, min(half, LANES // cap))
    small = (decay, query_gain, key_gain, norm_gain, routes, group_weight, inner_share)
    dma = pltpu.SemaphoreType.DMA
    rows = pltpu.VMEM((tok, width), jnp.bfloat16)
    info = pltpu.VMEM((INFO_ROWS, tok), jnp.float32)
    head_pairs = pltpu.VMEM((pairs, length, LANES), jnp.bfloat16)
    blocks = pltpu.VMEM((2, half, cap, width), jnp.bfloat16)
    sums = pltpu.VMEM((CHUNKS, tok, width // CHUNKS), jnp.bfloat16)
    flags = dma((2, CHUNKS, half))
    chunk_flags = dma((CHUNKS,))
    scratch = [pltpu.VMEM(array.shape, array.dtype) for array in small]
    scratch += [pltpu.VMEM(array.shape, array.dtype) for array in (gate, upper, down)]
    scratch += [rows, rows, info, dma((len(small),)), dma((3,))]
    attention_scratch = [
        rows,
        pltpu.VMEM((dp_size,) + out_weight.shape, jnp.bfloat16),
        rows,
        head_pairs,
        head_pairs,
        head_pairs,
        pltpu.VMEM((length, LANES), jnp.bfloat16),
        pltpu.VMEM((inner, length, LANES), jnp.bfloat16),
        pltpu.VMEM((length, 2 * LANES), jnp.bfloat16),
        head_pairs,
        dma((3, pairs)),
        dma((3, pairs, sp_size)),
        dma((3, pairs, sp_size)),
        dma((pairs,)),
        dma((pairs, sp_size)),
        dma((pairs, sp_size)),
        dma,
        dma((dp_size,)),
        dma((dp_size,)),
        dma((dp_size,)),
        dma((dp_size,)),
        dma,
    ]
    expert_scratch = [
        rows, info, blocks, blocks, blocks, blocks, sums, sums,
        dma((2,)), chunk_flags, chunk_flags,
        flags, flags, flags, flags,
        chunk_flags, chunk_flags,
    ]
    in_hbm = pl.BlockSpec(memory_space=pltpu.HBM)
    return pl.pallas_call(
        functools.partial(layer_kernel, sp_size, dp_size, head_size, per, top),
        out_shape=jax.ShapeDtypeStruct((tok, width), jnp.float32),
        in_specs=[in_hbm] * 15,
        out_specs=pl.BlockSpec(memory_space=pltpu.VMEM),
        scratch_shapes=scratch + attention_scratch + expert_scratch,
        compiler_params=pltpu.CompilerParams(
            collective_id=0, has_side_effects=True, vmem_limit_bytes=VMEM_LIMIT
        ),
        name="layer",
    )(queries, keys, values, out_weight, resid, gate, upper, down, *small)


VMEM_LIMIT = 62 * 1024 * 1024


def shards(
    resid,
    queries,
    keys,
    values,
    forget_cache,
    query_gain,
    key_gain,
    out_weight,
    norm_gain,
    routes,
    group_weight,
    inner_share,
    expert_gate,
    expert_up,
    expert_down,
):
    total = run_layer(
        queries[0], keys[0], values[0], out_weight, resid[0],
        expert_gate[0], expert_up[0], expert_down[0],
        forget_cache[0], query_gain[None], key_gain[None], norm_gain[None],
        routes[0].T, group_weight, inner_share[0].T,
    )
    return total.astype(jnp.bfloat16)[None]


def solution(mesh):
    return jax.shard_map(
        shards,
        mesh=mesh,
        in_specs=(
            P("dp", "sp", None),
            P("dp", "sp", None),
            P("dp", "sp", None),
            P("dp", "sp", None),
            P("dp", "sp", None),
            P(),
            P(),
            P(None, "dp"),
            P(),
            P("dp", "sp", None),
            P("dp", "sp"),
            P("dp", "sp", None),
            P(("sp", "dp"), None, None),
            P(("sp", "dp"), None, None),
            P(("sp", "dp"), None, None),
        ),
        out_specs=P("dp", "sp", None),
        check_vma=False,
    )
```

```python
import functools

import jax
import jax.numpy as jnp
from jax import lax
from jax.experimental import pallas as pl
from jax.experimental.pallas import tpu as pltpu
from jax.sharding import PartitionSpec as P

EPS = 1e-06


MESH = pl.DeviceIdType.MESH
LANES = 128
BLOCK = 256
DEPTH = 4


def place(index, size):
    return pl.ds(pl.multiple_of(index * size, size), size)


def half_means(squares, head_size):
    lane = lax.broadcasted_iota(jnp.int32, (LANES, LANES), 0) // head_size
    other = lax.broadcasted_iota(jnp.int32, (LANES, LANES), 1) // head_size
    same = (lane == other).astype(jnp.float32).astype(jnp.bfloat16)
    high = squares.astype(jnp.bfloat16)
    low = (squares - high.astype(jnp.float32)).astype(jnp.bfloat16)
    total = jnp.dot(high, same, preferred_element_type=jnp.float32)
    total = total + jnp.dot(low, same, preferred_element_type=jnp.float32)
    return total * (1.0 / head_size)


def attention_stage(
    n, dp_size, head_size, small_loads, weight_loads,
    q_ref, k_ref, v_ref, weight_ref, resid_ref,
    decay_ref, q_gain_ref, k_gain_ref, norm_gain_ref, routes_ref, group_ref, share_ref,
    mid_ref, normed_ref, info_ref, out_ref, weights, resid_buf,
    q_buf, k_buf, v_buf, q_norm, k_head, v_ones, o_buf,
    local_sem, send_sem, recv_sem, own_sem, back_send, back_recv,
    weight_sem, weight_send, weight_recv, pass_send, pass_recv, resid_sem,
    spread_send, spread_recv,
):
    me = lax.axis_index("sp")
    column = lax.axis_index("dp")
    rows_y = dp_size // 2
    row_y, core = column // 2, column % 2
    twin = row_y * 2 + 1 - core
    tok = q_ref.shape[0]
    pairs, length = q_buf.shape[0], q_buf.shape[1]
    inner = LANES // head_size
    sources, buffers = (q_ref, k_ref, v_ref), (q_buf, k_buf, v_buf)

    width_x = n // DEPTH
    x, plane_x = me % width_x, me - me % width_x
    rows = weight_ref.shape[0]
    share = rows // 2 // width_x

    def weight_rows(part):
        if part is None:
            return pl.ds(0, rows // 2)
        return pl.ds(pl.multiple_of(rows // 2 + part * share, share), share)

    def weight_block(step):
        return lax.rem(row_y + rows_y - step, rows_y) * 2 + core

    def weight_across(step, part, kind):
        return pltpu.make_async_remote_copy(
            src_ref=weight_ref.at[weight_rows(part), :],
            dst_ref=weights.at[column, weight_rows(part), :],
            send_sem=weight_send.at[kind, step],
            recv_sem=weight_recv.at[kind, step],
            device_id={"dp": lax.rem(row_y + step, rows_y) * 2 + core},
            device_id_type=MESH,
        )

    def weight_spread(step, turn, part):
        piece = weights.at[weight_block(step), weight_rows(part), :]
        return pltpu.make_async_remote_copy(
            src_ref=piece,
            dst_ref=piece,
            send_sem=spread_send.at[step, turn],
            recv_sem=spread_recv.at[step, turn],
            device_id={"sp": plane_x + lax.rem(x + turn, width_x)},
            device_id_type=MESH,
        )

    def weight_pass(step):
        block = weight_block(step)
        return pltpu.make_async_remote_copy(
            src_ref=weight_ref if step == 0 else weights.at[block],
            dst_ref=weights.at[block],
            send_sem=pass_send.at[step],
            recv_sem=pass_recv.at[step],
            device_id={"dp": twin},
            device_id_type=MESH,
        )

    weight_own = pltpu.make_async_copy(weight_ref, weights.at[column], weight_sem)

    def outgoing(kind, pair, step):
        target = lax.rem(me + step, n)
        return pltpu.make_async_remote_copy(
            src_ref=sources[kind].at[:, place(target * pairs + pair, LANES)],
            dst_ref=buffers[kind].at[pair, place(me, tok), :],
            send_sem=send_sem.at[kind],
            recv_sem=recv_sem.at[kind, pair],
            device_id={"sp": target},
            device_id_type=MESH,
        )

    def every_outgoing(kind, pair):
        view = buffers[kind].at[pair, pl.ds(0, (n - 1) * tok), :]
        return pltpu.make_async_remote_copy(
            src_ref=view, dst_ref=view, send_sem=send_sem.at[kind],
            recv_sem=recv_sem.at[kind, pair], device_id={"dp": twin}, device_id_type=MESH,
        )

    def own(kind, pair):
        return pltpu.make_async_copy(
            sources[kind].at[:, place(me * pairs + pair, LANES)],
            buffers[kind].at[pair, place(me, tok), :],
            local_sem.at[kind, pair],
        )

    def backward(pair, target):
        return pltpu.make_async_remote_copy(
            src_ref=o_buf.at[pair, pl.ds(target * tok, tok), :],
            dst_ref=out_ref.at[:, place(me * pairs + pair, LANES)],
            send_sem=back_send,
            recv_sem=back_recv,
            device_id={"sp": target},
            device_id_type=MESH,
        )

    def own_back(pair):
        return pltpu.make_async_copy(
            o_buf.at[pair, place(me, tok), :],
            out_ref.at[:, place(me * pairs + pair, LANES)],
            own_sem.at[pair],
        )

    for pair in range(pairs):
        for step in range(1, n):
            for kind in range(3):
                outgoing(kind, pair, step).start()
        for kind in range(3):
            own(kind, pair).start()

    for step in range(1, rows_y):
        weight_across(step, x, 0).start()
    for step in range(1, rows_y):
        weight_across(step, None, 1).start()
    weight_pass(0).start()
    weight_own.start()
    load_resid = pltpu.make_async_copy(resid_ref, resid_buf, resid_sem)
    load_resid.start()
    for load in weight_loads:
        load.start()
    for load in small_loads:
        load.wait()
    info_ref[...] = routing_info(routes_ref, group_ref, share_ref, n * dp_size)
    q_gain = jnp.concatenate([q_gain_ref[...]] * inner, axis=1)
    k_gain = jnp.concatenate([k_gain_ref[...]] * inner, axis=1)

    row = lax.broadcasted_iota(jnp.int32, (BLOCK, BLOCK), 0)
    col = lax.broadcasted_iota(jnp.int32, (BLOCK, BLOCK), 1)
    lane = lax.broadcasted_iota(jnp.int32, (length, LANES), 1) // head_size
    out_lane = lax.broadcasted_iota(jnp.int32, (BLOCK, LANES), 1) // head_size
    scale = head_size ** (-0.5)
    v_ones[:, LANES:] = jnp.ones((length, LANES), jnp.bfloat16)

    def scores_of(queries, keys):
        return lax.dot_general(
            queries, keys, (((1,), (1,)), ((), ())), preferred_element_type=jnp.float32
        )

    def one_pair(pair, carry):
        for kind in range(3):
            own(kind, pair).wait()
            every_outgoing(kind, pair).wait_recv()
        floats = q_buf[pair].astype(jnp.float32)
        floats = floats * lax.rsqrt(half_means(floats * floats, head_size) + EPS)
        normed = (floats * q_gain).astype(jnp.bfloat16)
        q_norm[...] = (normed.astype(jnp.float32) * scale).astype(jnp.bfloat16)
        floats = k_buf[pair].astype(jnp.float32)
        floats = floats * lax.rsqrt(half_means(floats * floats, head_size) + EPS)
        floats = floats * k_gain
        for head in range(inner):
            k_head[head] = jnp.where(lane == head, floats, 0.0).astype(jnp.bfloat16)
        v_ones[:, :LANES] = v_buf[pair]
        for block in range(length // BLOCK):
            first = block * BLOCK
            here = slice(first, first + BLOCK)
            query_block = q_norm[here, :]
            merged = None
            for head in range(inner):
                decay = decay_ref[pl.ds(pair * inner + head, 1), :]
                decay_here = decay[:, here]
                query_decay = jnp.sum(
                    jnp.where(row == col, decay_here, 0.0), axis=1, keepdims=True
                )
                near = scores_of(query_block, k_head[head, here, :])
                near = near + (query_decay - decay_here)
                near = jnp.where(col <= row, near, -jnp.inf)
                highest = jnp.max(near, axis=1, keepdims=True)
                if block > 0:
                    far = scores_of(query_block, k_head[head, :first, :])
                    far = far + (query_decay - decay[:, :first])
                    highest = jnp.maximum(highest, jnp.max(far, axis=1, keepdims=True))
                total = jnp.dot(
                    jnp.exp(near - highest).astype(jnp.bfloat16),
                    v_ones[here, :],
                    preferred_element_type=jnp.float32,
                )
                if block > 0:
                    total = total + jnp.dot(
                        jnp.exp(far - highest).astype(jnp.bfloat16),
                        v_ones[:first, :],
                        preferred_element_type=jnp.float32,
                    )
                result = total[:, :LANES] / total[:, LANES:]
                merged = result if head == 0 else jnp.where(out_lane == head, result, merged)
            o_buf[pair, here, :] = merged.astype(jnp.bfloat16)
            for target in range(first // tok, (first + BLOCK) // tok):
                @pl.when(target == me)
                def _():
                    own_back(pair).start()

                @pl.when(target != me)
                def _():
                    backward(pair, target).start()

        @pl.when(pair == 0)
        def _():
            for step in range(1, rows_y):
                weight_across(step, x, 0).wait_recv()
                for turn in range(1, width_x):
                    weight_spread(step, turn, x).start()

        return carry

    lax.fori_loop(0, pairs, one_pair, 0)
    for step in range(1, rows_y):
        weight_across(step, None, 1).wait_recv()
        for turn in range(1, width_x):
            weight_spread(step, turn, lax.rem(x + width_x - turn, width_x)).wait_recv()
        weight_pass(step).start()

    def finish(pair, carry):
        own_back(pair).wait()
        for kind in range(3):
            every_outgoing(kind, pair).wait_send()
        return carry

    lax.fori_loop(0, pairs, finish, 0)
    every_back = pltpu.make_async_remote_copy(
        src_ref=o_buf.at[:, pl.ds(0, (n - 1) * tok), :],
        dst_ref=out_ref.at[:, pl.ds(0, (n - 1) * pairs * LANES)],
        send_sem=back_send, recv_sem=back_recv, device_id={"dp": twin}, device_id_type=MESH,
    )
    every_back.wait()
    weight_own.wait()
    for step in range(1, rows_y):
        weight_across(step, x, 0).wait_send()
        weight_across(step, None, 1).wait_send()
        for turn in range(1, width_x):
            weight_spread(step, turn, x).wait_send()
    for step in range(rows_y):
        weight_pass(step).wait()
    load_resid.wait()
    span = weights.shape[2]
    squares = jnp.zeros((tok, 1), jnp.float32)
    for block in range(dp_size):
        columns = slice(block * span, (block + 1) * span)
        projected = jnp.dot(
            out_ref[...], weights[block], preferred_element_type=jnp.float32
        )
        mid = (resid_buf[:, columns].astype(jnp.float32) + projected).astype(jnp.bfloat16)
        mid_ref[:, columns] = mid
        floats = mid.astype(jnp.float32)
        squares = squares + jnp.sum(floats * floats, axis=1, keepdims=True)
    factor = lax.rsqrt(squares * (1.0 / (dp_size * span)) + EPS)
    for block in range(dp_size):
        columns = slice(block * span, (block + 1) * span)
        scaled = mid_ref[:, columns].astype(jnp.float32) * factor
        normed_ref[:, columns] = (scaled * norm_gain_ref[:, columns]).astype(jnp.bfloat16)


INFO_ROWS = 8


def routing_info(routes_ref, group_ref, share_ref, experts):
    top, tok = routes_ref.shape
    capacity = 2 * tok * top // experts
    expert = lax.broadcasted_iota(jnp.int32, (experts, tok), 0)
    hits = [(expert == routes_ref[r : r + 1, :]).astype(jnp.float32) for r in range(top)]
    every = sum(hits[1:], hits[0]).astype(jnp.bfloat16)
    row = lax.broadcasted_iota(jnp.int32, (tok, tok), 0)
    col = lax.broadcasted_iota(jnp.int32, (tok, tok), 1)
    before = (row < col).astype(jnp.float32).astype(jnp.bfloat16)
    earlier = jnp.dot(every, before, preferred_element_type=jnp.float32)
    shares = [share_ref[r : r + 1, :] for r in range(top)]
    total = sum(shares[1:], shares[0])
    lines = [
        routes_ref[r : r + 1, :].astype(jnp.float32) * capacity
        + jnp.sum(hits[r] * earlier, axis=0, keepdims=True)
        for r in range(top)
    ]
    lines += [group_ref[...] * shares[r] / total for r in range(top)]
    lines.append(jnp.zeros((INFO_ROWS - 2 * top, tok), jnp.float32))
    return jnp.concatenate(lines, axis=0)


CHUNKS = 4


def expert_stage(
    sp_size, dp_size, per, top, weight_loads,
    mid_ref, normed_ref, info_ref, gate_buf, up_buf, down_buf,
    out_ref,
    far_rows, far_info, packed, arrived, result, returned, partial, incoming,
    info_sem, row_send, row_recv, send_sem, recv_sem,
    back_send, back_recv, sum_send, sum_recv,
):
    n = sp_size * dp_size
    half = n // 2
    me = lax.axis_index("sp") * dp_size + lax.axis_index("dp")
    side, seat = me // half, me % half
    twin = (me + half) % n
    tok, width = normed_ref.shape
    cap = packed.shape[2]
    part = width // CHUNKS
    mine = half // 2

    def columns(chunk):
        return slice(chunk * part, (chunk + 1) * part)

    def coords(flat):
        return {"sp": flat // dp_size, "dp": flat % dp_size}

    info_copy = pltpu.make_async_remote_copy(
        src_ref=info_ref, dst_ref=far_info, send_sem=info_sem.at[0], recv_sem=info_sem.at[1],
        device_id=coords(twin), device_id_type=MESH,
    )
    row_copies = [
        pltpu.make_async_remote_copy(
            src_ref=normed_ref.at[:, columns(chunk)],
            dst_ref=far_rows.at[:, columns(chunk)],
            send_sem=row_send.at[chunk],
            recv_sem=row_recv.at[chunk],
            device_id=coords(twin),
            device_id_type=MESH,
        )
        for chunk in range(CHUNKS)
    ]

    def outgoing(kind, step, chunk):
        target = (seat + mine + step) % half
        return pltpu.make_async_remote_copy(
            src_ref=packed.at[kind, target, :, columns(chunk)],
            dst_ref=arrived.at[kind, step, :, columns(chunk)],
            send_sem=send_sem.at[kind],
            recv_sem=recv_sem.at[kind, step // per],
            device_id=coords(side * half + target),
            device_id_type=MESH,
        )

    def backward(kind, step, chunk):
        target = (seat + half + half - mine - step) % half
        return pltpu.make_async_remote_copy(
            src_ref=result.at[kind, step, :, columns(chunk)],
            dst_ref=returned.at[kind, seat, :, columns(chunk)],
            send_sem=back_send.at[kind],
            recv_sem=back_recv.at[kind, chunk],
            device_id=coords(side * half + target),
            device_id_type=MESH,
        )

    def dummy(view, sent, received):
        return pltpu.make_async_remote_copy(
            src_ref=view, dst_ref=view, send_sem=sent, recv_sem=received,
            device_id=coords(twin), device_id_type=MESH,
        )

    def sum_copy(chunk):
        return pltpu.make_async_remote_copy(
            src_ref=partial.at[chunk],
            dst_ref=incoming.at[chunk],
            send_sem=sum_send.at[chunk],
            recv_sem=sum_recv.at[chunk],
            device_id=coords(twin),
            device_id_type=MESH,
        )

    def others(action, start=0, stop=half):
        def run(step, carry):
            @pl.when(step != mine)
            def _():
                action(step)

            return carry

        lax.fori_loop(start, stop, run, 0)

    first_slot = (side * (half * cap)).astype(jnp.float32)

    def dispatch(kind, source_ref, route_ref, chunk):
        slot = lax.broadcasted_iota(jnp.int32, (half * cap, tok), 0).astype(jnp.float32)
        hit = jnp.zeros((half * cap, tok), jnp.float32)
        for route in range(top):
            local = route_ref[route : route + 1, :] - first_slot
            hit = hit + jnp.where(slot == local, 1.0, 0.0)
        rows = jnp.dot(
            hit.astype(jnp.bfloat16), source_ref[:, columns(chunk)],
            preferred_element_type=jnp.float32,
        )
        packed[kind, :, :, columns(chunk)] = rows.astype(jnp.bfloat16).reshape(half, cap, part)
        others(lambda step: outgoing(kind, step, chunk).start())
        arrived[kind, mine, :, columns(chunk)] = packed[kind, seat, :, columns(chunk)]

    def forward(kind, send_back):
        def group(index, carry):
            first = index * per

            sent, received = send_sem.at[kind], recv_sem.at[kind, index]

            @pl.when(first == mine)
            def _():
                dummy(arrived.at[kind, pl.ds(first + 1, per - 1)], sent, received).wait_recv()

            @pl.when(first != mine)
            def _():
                dummy(arrived.at[kind, pl.ds(first, per)], sent, received).wait_recv()

            rows = arrived[kind, pl.ds(first, per)].reshape(per * cap, width)
            gate = jnp.dot(rows, gate_buf[...], preferred_element_type=jnp.float32)
            upper = jnp.dot(rows, up_buf[...], preferred_element_type=jnp.float32)
            hidden = (gate / (1.0 + jnp.exp(-gate)) * upper).astype(jnp.bfloat16)
            for chunk in range(CHUNKS):
                product = jnp.dot(
                    hidden, down_buf[:, columns(chunk)], preferred_element_type=jnp.float32
                )
                result[kind, pl.ds(first, per), :, columns(chunk)] = product.astype(
                    jnp.bfloat16
                ).reshape(per, cap, part)
                if send_back:
                    others(lambda step: backward(kind, step, chunk).start(), first, first + per)
            return carry

        lax.fori_loop(0, half // per, group, 0)
        returned[kind, seat] = result[kind, mine]

    row = lax.broadcasted_iota(jnp.int32, (tok, tok), 0)
    col = lax.broadcasted_iota(jnp.int32, (tok, tok), 1)

    def upright(line):
        return jnp.sum(jnp.where(row == col, line, 0.0), axis=1, keepdims=True)

    def choices(route_ref):
        slot = lax.broadcasted_iota(jnp.int32, (tok, half * cap), 1).astype(jnp.float32)
        picks = []
        for route in range(top):
            local = upright(route_ref[route : route + 1, :]) - first_slot
            pick = jnp.where(slot == local, 1.0, 0.0).astype(jnp.bfloat16)
            picks.append((pick, upright(route_ref[top + route : top + route + 1, :])))
        return picks

    def combine(kind, picks, chunk):
        view = returned.at[kind, pl.ds(0, half - 1), :, columns(chunk)]
        dummy(view, back_send.at[kind], back_recv.at[kind, chunk]).wait_recv()
        block = returned[kind, :, :, columns(chunk)].reshape(half * cap, part)
        total = None
        for pick, weight in picks:
            term = weight * jnp.dot(pick, block, preferred_element_type=jnp.float32)
            total = term if total is None else total + term
        return total

    info_copy.start()
    for copy in row_copies:
        copy.start()
    for chunk in range(CHUNKS):
        dispatch(0, normed_ref, info_ref, chunk)
    info_copy.wait_recv()
    for chunk in range(CHUNKS):
        row_copies[chunk].wait_recv()
        dispatch(1, far_rows, far_info, chunk)
    for load in weight_loads:
        load.wait()
    forward(0, False)
    forward(1, True)
    for chunk in range(CHUNKS):
        others(lambda step: backward(0, step, chunk).start())
    far_picks = choices(far_info)
    for chunk in range(CHUNKS):
        partial[chunk] = combine(1, far_picks, chunk).astype(jnp.bfloat16)
        sum_copy(chunk).start()
    picks = choices(info_ref)
    for chunk in range(CHUNKS):
        total = combine(0, picks, chunk)
        sum_copy(chunk).wait_recv()
        total = total + incoming[chunk].astype(jnp.float32)
        out_ref[:, columns(chunk)] = mid_ref[:, columns(chunk)].astype(jnp.float32) + total

    info_copy.wait_send()
    for chunk in range(CHUNKS):
        row_copies[chunk].wait_send()
        sum_copy(chunk).wait_send()

    for kind in range(2):
        whole = pl.ds(0, half - 1)
        dummy(packed.at[kind, whole], send_sem.at[kind], recv_sem.at[kind, 0]).wait_send()
        dummy(result.at[kind, whole], back_send.at[kind], back_recv.at[kind, 0]).wait_send()


def layer_kernel(sp_size, dp_size, head_size, per, top, *refs):
    inputs, out_ref, scratch = refs[:15], refs[15], refs[16:]
    (
        q_ref, k_ref, v_ref, weight_ref, resid_ref, gate_ref, up_ref, down_ref,
    ) = inputs[:8]
    small = scratch[:7]
    gate_buf, up_buf, down_buf, mid_ref, normed_ref, info_ref = scratch[7:13]
    small_sem, load_sem = scratch[13:15]
    attention_scratch, expert_scratch = scratch[15:39], scratch[39:]
    small_loads = [
        pltpu.make_async_copy(source, target, small_sem.at[index])
        for index, (source, target) in enumerate(zip(inputs[8:], small))
    ]
    weight_loads = [
        pltpu.make_async_copy(source, target, load_sem.at[index])
        for index, (source, target) in enumerate(
            ((gate_ref, gate_buf), (up_ref, up_buf), (down_ref, down_buf))
        )
    ]
    for load in small_loads:
        load.start()
    n = sp_size * dp_size
    me = lax.axis_index("sp") * dp_size + lax.axis_index("dp")
    barrier = pltpu.get_barrier_semaphore()

    def greet(step, carry):
        other = (me + step) % n
        pl.semaphore_signal(
            barrier, inc=1, device_id={"sp": other // dp_size, "dp": other % dp_size},
            device_id_type=MESH,
        )
        return carry

    lax.fori_loop(1, n, greet, 0)
    pl.semaphore_wait(barrier, n - 1)
    attention_stage(
        sp_size, dp_size, head_size, small_loads, weight_loads,
        q_ref, k_ref, v_ref, weight_ref, resid_ref, *small,
        mid_ref, normed_ref, info_ref, *attention_scratch,
    )
    expert_stage(
        sp_size, dp_size, per, top, weight_loads,
        mid_ref, normed_ref, info_ref, gate_buf, up_buf, down_buf, out_ref, *expert_scratch,
    )


def run_layer(
    queries, keys, values, out_weight, resid, gate, upper, down,
    decay, query_gain, key_gain, norm_gain, routes, group_weight, inner_share,
):
    tok, width = queries.shape
    sp_size, dp_size = lax.axis_size("sp"), lax.axis_size("dp")
    top = routes.shape[0]
    head_size = query_gain.shape[1]
    inner = LANES // head_size
    pairs = width // sp_size // LANES
    length = sp_size * tok
    n = sp_size * dp_size
    half = n // 2
    cap = 2 * tok * top // n
    per = max(1, min(half // 2, LANES // cap))
    small = (decay, query_gain, key_gain, norm_gain, routes, group_weight, inner_share)
    dma = pltpu.SemaphoreType.DMA
    rows = pltpu.VMEM((tok, width), jnp.bfloat16)
    info = pltpu.VMEM((INFO_ROWS, tok), jnp.float32)
    head_pairs = pltpu.VMEM((pairs, length, LANES), jnp.bfloat16)
    blocks = pltpu.VMEM((2, half, cap, width), jnp.bfloat16)
    sums = pltpu.VMEM((CHUNKS, tok, width // CHUNKS), jnp.bfloat16)
    chunk_flags = dma((CHUNKS,))
    scratch = [pltpu.VMEM(array.shape, array.dtype) for array in small]
    scratch += [pltpu.VMEM(array.shape, array.dtype) for array in (gate, upper, down)]
    scratch += [rows, rows, info, dma((len(small),)), dma((3,))]
    attention_scratch = [
        rows,
        pltpu.VMEM((dp_size,) + out_weight.shape, jnp.bfloat16),
        rows,
        head_pairs,
        head_pairs,
        head_pairs,
        pltpu.VMEM((length, LANES), jnp.bfloat16),
        pltpu.VMEM((inner, length, LANES), jnp.bfloat16),
        pltpu.VMEM((length, 2 * LANES), jnp.bfloat16),
        head_pairs,
        dma((3, pairs)),
        dma((3,)),
        dma((3, pairs)),
        dma((pairs,)),
        dma,
        dma,
        dma,
        dma((2, dp_size // 2)),
        dma((2, dp_size // 2)),
        dma((dp_size // 2,)),
        dma((dp_size // 2,)),
        dma,
        dma((dp_size // 2, sp_size // DEPTH)),
        dma((dp_size // 2, sp_size // DEPTH)),
    ]
    expert_scratch = [
        rows, info, blocks, blocks, blocks, blocks, sums, sums,
        dma((2,)), chunk_flags, chunk_flags,
        dma((2,)), dma((2, half // per)), dma((2,)), dma((2, CHUNKS)),
        chunk_flags, chunk_flags,
    ]
    in_hbm = pl.BlockSpec(memory_space=pltpu.HBM)
    return pl.pallas_call(
        functools.partial(layer_kernel, sp_size, dp_size, head_size, per, top),
        out_shape=jax.ShapeDtypeStruct((tok, width), jnp.float32),
        in_specs=[in_hbm] * 15,
        out_specs=pl.BlockSpec(memory_space=pltpu.VMEM),
        scratch_shapes=scratch + attention_scratch + expert_scratch,
        compiler_params=pltpu.CompilerParams(
            collective_id=0, has_side_effects=True, vmem_limit_bytes=VMEM_LIMIT
        ),
        name="layer",
    )(queries, keys, values, out_weight, resid, gate, upper, down, *small)


VMEM_LIMIT = 62 * 1024 * 1024


def shards(
    resid,
    queries,
    keys,
    values,
    forget_cache,
    query_gain,
    key_gain,
    out_weight,
    norm_gain,
    routes,
    group_weight,
    inner_share,
    expert_gate,
    expert_up,
    expert_down,
):
    total = run_layer(
        queries[0], keys[0], values[0], out_weight, resid[0],
        expert_gate[0], expert_up[0], expert_down[0],
        forget_cache[0], query_gain[None], key_gain[None], norm_gain[None],
        routes[0].T, group_weight, inner_share[0].T,
    )
    return total.astype(jnp.bfloat16)[None]


def solution(mesh):
    return jax.shard_map(
        shards,
        mesh=mesh,
        in_specs=(
            P("dp", "sp", None),
            P("dp", "sp", None),
            P("dp", "sp", None),
            P("dp", "sp", None),
            P("dp", "sp", None),
            P(),
            P(),
            P(None, "dp"),
            P(),
            P("dp", "sp", None),
            P("dp", "sp"),
            P("dp", "sp", None),
            P(("sp", "dp"), None, None),
            P(("sp", "dp"), None, None),
            P(("sp", "dp"), None, None),
        ),
        out_specs=P("dp", "sp", None),
        check_vma=False,
    )
```

```python
import functools

import jax
import jax.numpy as jnp
from jax import lax
from jax.experimental import pallas as pl
from jax.experimental.pallas import tpu as pltpu
from jax.sharding import PartitionSpec as P

EPS = 1e-06


MESH = pl.DeviceIdType.MESH
LANES = 128
BLOCK = 256
DEPTH = 4


def place(index, size):
    return pl.ds(pl.multiple_of(index * size, size), size)


def half_means(squares, head_size):
    lane = lax.broadcasted_iota(jnp.int32, (LANES, LANES), 0) // head_size
    other = lax.broadcasted_iota(jnp.int32, (LANES, LANES), 1) // head_size
    same = (lane == other).astype(jnp.float32).astype(jnp.bfloat16)
    high = squares.astype(jnp.bfloat16)
    low = (squares - high.astype(jnp.float32)).astype(jnp.bfloat16)
    total = jnp.dot(high, same, preferred_element_type=jnp.float32)
    total = total + jnp.dot(low, same, preferred_element_type=jnp.float32)
    return total * (1.0 / head_size)


def attention_stage(
    n, dp_size, head_size, weight_loads,
    q_ref, k_ref, v_ref, weight_ref, resid_ref,
    decay_ref, q_gain_ref, k_gain_ref, norm_gain_ref, routes_ref, group_ref, share_ref,
    mid_ref, normed_ref, info_ref, out_ref, weights, resid_buf,
    q_buf, k_buf, v_buf, k_head, v_ones, o_buf,
    local_sem, send_sem, recv_sem, own_sem, back_send, back_recv,
    weight_sem, weight_send, weight_recv, pass_send, pass_recv, resid_sem,
    spread_send, spread_recv,
):
    me = lax.axis_index("sp")
    column = lax.axis_index("dp")
    rows_y = dp_size // 2
    row_y, core = column // 2, column % 2
    twin = row_y * 2 + 1 - core
    tok = q_ref.shape[0]
    pairs, length = q_buf.shape[0], q_buf.shape[1]
    inner = LANES // head_size
    sources, buffers = (q_ref, k_ref, v_ref), (q_buf, k_buf, v_buf)

    width_x = n // DEPTH
    x, plane_x = me % width_x, me - me % width_x
    rows = weight_ref.shape[0]
    share = rows // 2 // width_x

    def weight_rows(part):
        if part is None:
            return pl.ds(0, rows // 2)
        return pl.ds(pl.multiple_of(rows // 2 + part * share, share), share)

    def weight_block(step):
        return lax.rem(row_y + rows_y - step, rows_y) * 2 + core

    def weight_across(step, part, kind):
        return pltpu.make_async_remote_copy(
            src_ref=weight_ref.at[weight_rows(part), :],
            dst_ref=weights.at[column, weight_rows(part), :],
            send_sem=weight_send.at[kind, step],
            recv_sem=weight_recv.at[kind, step],
            device_id={"dp": lax.rem(row_y + step, rows_y) * 2 + core},
            device_id_type=MESH,
        )

    def weight_spread(step, turn, part):
        piece = weights.at[weight_block(step), weight_rows(part), :]
        return pltpu.make_async_remote_copy(
            src_ref=piece,
            dst_ref=piece,
            send_sem=spread_send.at[step, turn],
            recv_sem=spread_recv.at[step, turn],
            device_id={"sp": plane_x + lax.rem(x + turn, width_x)},
            device_id_type=MESH,
        )

    def weight_pass(step):
        block = weight_block(step)
        return pltpu.make_async_remote_copy(
            src_ref=weight_ref if step == 0 else weights.at[block],
            dst_ref=weights.at[block],
            send_sem=pass_send.at[step],
            recv_sem=pass_recv.at[step],
            device_id={"dp": twin},
            device_id_type=MESH,
        )

    weight_own = pltpu.make_async_copy(weight_ref, weights.at[column], weight_sem)

    def outgoing(kind, pair, step):
        target = lax.rem(me + step, n)
        return pltpu.make_async_remote_copy(
            src_ref=sources[kind].at[:, place(target * pairs + pair, LANES)],
            dst_ref=buffers[kind].at[pair, place(me, tok), :],
            send_sem=send_sem.at[kind],
            recv_sem=recv_sem.at[kind, pair],
            device_id={"sp": target},
            device_id_type=MESH,
        )

    def every_outgoing(kind, pair):
        view = buffers[kind].at[pair, pl.ds(0, (n - 1) * tok), :]
        return pltpu.make_async_remote_copy(
            src_ref=view, dst_ref=view, send_sem=send_sem.at[kind],
            recv_sem=recv_sem.at[kind, pair], device_id={"dp": twin}, device_id_type=MESH,
        )

    def own(kind, pair):
        return pltpu.make_async_copy(
            sources[kind].at[:, place(me * pairs + pair, LANES)],
            buffers[kind].at[pair, place(me, tok), :],
            local_sem.at[kind, pair],
        )

    def backward(pair, target):
        return pltpu.make_async_remote_copy(
            src_ref=o_buf.at[pair, pl.ds(target * tok, tok), :],
            dst_ref=out_ref.at[:, place(me * pairs + pair, LANES)],
            send_sem=back_send,
            recv_sem=back_recv,
            device_id={"sp": target},
            device_id_type=MESH,
        )

    def own_back(pair):
        return pltpu.make_async_copy(
            o_buf.at[pair, place(me, tok), :],
            out_ref.at[:, place(me * pairs + pair, LANES)],
            own_sem.at[pair],
        )

    for pair in range(pairs):
        for step in range(1, n):
            for kind in range(3):
                outgoing(kind, pair, step).start()
        for kind in range(3):
            own(kind, pair).start()

    for step in range(1, rows_y):
        weight_across(step, x, 0).start()
    for step in range(1, rows_y):
        weight_across(step, None, 1).start()
    weight_pass(0).start()
    weight_own.start()
    load_resid = pltpu.make_async_copy(resid_ref, resid_buf, resid_sem)
    load_resid.start()
    for load in weight_loads:
        load.start()
    info_ref[...] = routing_info(routes_ref, group_ref, share_ref, n * dp_size)
    row = lax.broadcasted_iota(jnp.int32, (BLOCK, BLOCK), 0)
    col = lax.broadcasted_iota(jnp.int32, (BLOCK, BLOCK), 1)
    lane = lax.broadcasted_iota(jnp.int32, (length, LANES), 1) // head_size
    out_lane = lax.broadcasted_iota(jnp.int32, (BLOCK, LANES), 1) // head_size
    v_ones[:, LANES:] = jnp.ones((length, LANES), jnp.bfloat16)

    def scores_of(queries, keys):
        return lax.dot_general(
            queries, keys, (((1,), (1,)), ((), ())), preferred_element_type=jnp.float32
        )

    def one_pair(pair, carry):
        for kind in range(3):
            own(kind, pair).wait()
            every_outgoing(kind, pair).wait_recv()
        floats = k_buf[pair].astype(jnp.float32)
        for head in range(inner):
            k_head[head] = jnp.where(lane == head, floats, 0.0).astype(jnp.bfloat16)
        v_ones[:, :LANES] = v_buf[pair]
        for block in range(length // BLOCK):
            first = block * BLOCK
            here = slice(first, first + BLOCK)
            query_block = q_buf[pair, here, :]
            merged = None
            for head in range(inner):
                decay = decay_ref[pl.ds(pair * inner + head, 1), :]
                decay_here = decay[:, here]
                query_decay = jnp.sum(
                    jnp.where(row == col, decay_here, 0.0), axis=1, keepdims=True
                )
                near = scores_of(query_block, k_head[head, here, :])
                near = near + (query_decay - decay_here)
                near = jnp.where(col <= row, near, -jnp.inf)
                highest = jnp.max(near, axis=1, keepdims=True)
                if block > 0:
                    far = scores_of(query_block, k_head[head, :first, :])
                    far = far + (query_decay - decay[:, :first])
                    highest = jnp.maximum(highest, jnp.max(far, axis=1, keepdims=True))
                total = jnp.dot(
                    jnp.exp(near - highest).astype(jnp.bfloat16),
                    v_ones[here, :],
                    preferred_element_type=jnp.float32,
                )
                if block > 0:
                    total = total + jnp.dot(
                        jnp.exp(far - highest).astype(jnp.bfloat16),
                        v_ones[:first, :],
                        preferred_element_type=jnp.float32,
                    )
                result = total[:, :LANES] / total[:, LANES:]
                merged = result if head == 0 else jnp.where(out_lane == head, result, merged)
            o_buf[pair, here, :] = merged.astype(jnp.bfloat16)
            for target in range(first // tok, (first + BLOCK) // tok):
                @pl.when(target == me)
                def _():
                    own_back(pair).start()

                @pl.when(target != me)
                def _():
                    backward(pair, target).start()

        @pl.when(pair == 0)
        def _():
            for step in range(1, rows_y):
                weight_across(step, x, 0).wait_recv()
                for turn in range(1, width_x):
                    weight_spread(step, turn, x).start()

        return carry

    lax.fori_loop(0, pairs, one_pair, 0)
    for step in range(1, rows_y):
        weight_across(step, None, 1).wait_recv()
        for turn in range(1, width_x):
            weight_spread(step, turn, lax.rem(x + width_x - turn, width_x)).wait_recv()
        weight_pass(step).start()

    def finish(pair, carry):
        own_back(pair).wait()
        for kind in range(3):
            every_outgoing(kind, pair).wait_send()
        return carry

    lax.fori_loop(0, pairs, finish, 0)
    every_back = pltpu.make_async_remote_copy(
        src_ref=o_buf.at[:, pl.ds(0, (n - 1) * tok), :],
        dst_ref=out_ref.at[:, pl.ds(0, (n - 1) * pairs * LANES)],
        send_sem=back_send, recv_sem=back_recv, device_id={"dp": twin}, device_id_type=MESH,
    )
    every_back.wait()
    weight_own.wait()
    for step in range(1, rows_y):
        weight_across(step, x, 0).wait_send()
        weight_across(step, None, 1).wait_send()
        for turn in range(1, width_x):
            weight_spread(step, turn, x).wait_send()
    for step in range(rows_y):
        weight_pass(step).wait()
    load_resid.wait()
    span = weights.shape[2]
    squares = jnp.zeros((tok, 1), jnp.float32)
    for block in range(dp_size):
        columns = slice(block * span, (block + 1) * span)
        projected = jnp.dot(
            out_ref[...], weights[block], preferred_element_type=jnp.float32
        )
        mid = (resid_buf[:, columns].astype(jnp.float32) + projected).astype(jnp.bfloat16)
        mid_ref[:, columns] = mid
        floats = mid.astype(jnp.float32)
        squares = squares + jnp.sum(floats * floats, axis=1, keepdims=True)
    factor = lax.rsqrt(squares * (1.0 / (dp_size * span)) + EPS)
    for block in range(dp_size):
        columns = slice(block * span, (block + 1) * span)
        scaled = mid_ref[:, columns].astype(jnp.float32) * factor
        normed_ref[:, columns] = (scaled * norm_gain_ref[:, columns]).astype(jnp.bfloat16)


INFO_ROWS = 8


def routing_info(routes_ref, group_ref, share_ref, experts):
    top, tok = routes_ref.shape
    capacity = 2 * tok * top // experts
    expert = lax.broadcasted_iota(jnp.int32, (experts, tok), 0)
    hits = [(expert == routes_ref[r : r + 1, :]).astype(jnp.float32) for r in range(top)]
    every = sum(hits[1:], hits[0]).astype(jnp.bfloat16)
    row = lax.broadcasted_iota(jnp.int32, (tok, tok), 0)
    col = lax.broadcasted_iota(jnp.int32, (tok, tok), 1)
    before = (row < col).astype(jnp.float32).astype(jnp.bfloat16)
    earlier = jnp.dot(every, before, preferred_element_type=jnp.float32)
    shares = [share_ref[r : r + 1, :] for r in range(top)]
    total = sum(shares[1:], shares[0])
    lines = [
        routes_ref[r : r + 1, :].astype(jnp.float32) * capacity
        + jnp.sum(hits[r] * earlier, axis=0, keepdims=True)
        for r in range(top)
    ]
    lines += [group_ref[...] * shares[r] / total for r in range(top)]
    lines.append(jnp.zeros((INFO_ROWS - 2 * top, tok), jnp.float32))
    return jnp.concatenate(lines, axis=0)


CHUNKS = 4


def expert_stage(
    sp_size, dp_size, per, top, weight_loads,
    mid_ref, normed_ref, info_ref, gate_buf, up_buf, down_buf,
    out_ref,
    far_rows, far_info, packed, arrived, result, returned, partial, incoming,
    info_sem, row_send, row_recv, send_sem, recv_sem,
    back_send, back_recv, sum_send, sum_recv,
):
    n = sp_size * dp_size
    half = n // 2
    me = lax.axis_index("sp") * dp_size + lax.axis_index("dp")
    side, seat = me // half, me % half
    twin = (me + half) % n
    tok, width = normed_ref.shape
    cap = packed.shape[2]
    part = width // CHUNKS
    mine = half // 2

    def columns(chunk):
        return slice(chunk * part, (chunk + 1) * part)

    def coords(flat):
        return {"sp": flat // dp_size, "dp": flat % dp_size}

    info_copy = pltpu.make_async_remote_copy(
        src_ref=info_ref, dst_ref=far_info, send_sem=info_sem.at[0], recv_sem=info_sem.at[1],
        device_id=coords(twin), device_id_type=MESH,
    )
    row_copies = [
        pltpu.make_async_remote_copy(
            src_ref=normed_ref.at[:, columns(chunk)],
            dst_ref=far_rows.at[:, columns(chunk)],
            send_sem=row_send.at[chunk],
            recv_sem=row_recv.at[chunk],
            device_id=coords(twin),
            device_id_type=MESH,
        )
        for chunk in range(CHUNKS)
    ]

    def outgoing(kind, step, chunk):
        target = (seat + mine + step) % half
        return pltpu.make_async_remote_copy(
            src_ref=packed.at[kind, target, :, columns(chunk)],
            dst_ref=arrived.at[kind, step, :, columns(chunk)],
            send_sem=send_sem.at[kind],
            recv_sem=recv_sem.at[kind, step // per],
            device_id=coords(side * half + target),
            device_id_type=MESH,
        )

    def backward(kind, step, chunk):
        target = (seat + half + half - mine - step) % half
        return pltpu.make_async_remote_copy(
            src_ref=result.at[kind, step, :, columns(chunk)],
            dst_ref=returned.at[kind, seat, :, columns(chunk)],
            send_sem=back_send.at[kind],
            recv_sem=back_recv.at[kind, chunk],
            device_id=coords(side * half + target),
            device_id_type=MESH,
        )

    def dummy(view, sent, received):
        return pltpu.make_async_remote_copy(
            src_ref=view, dst_ref=view, send_sem=sent, recv_sem=received,
            device_id=coords(twin), device_id_type=MESH,
        )

    def sum_copy(chunk):
        return pltpu.make_async_remote_copy(
            src_ref=partial.at[chunk],
            dst_ref=incoming.at[chunk],
            send_sem=sum_send.at[chunk],
            recv_sem=sum_recv.at[chunk],
            device_id=coords(twin),
            device_id_type=MESH,
        )

    def others(action, start=0, stop=half):
        def run(step, carry):
            @pl.when(step != mine)
            def _():
                action(step)

            return carry

        lax.fori_loop(start, stop, run, 0)

    first_slot = (side * (half * cap)).astype(jnp.float32)

    def dispatch(kind, source_ref, route_ref, chunk):
        slot = lax.broadcasted_iota(jnp.int32, (half * cap, tok), 0).astype(jnp.float32)
        hit = jnp.zeros((half * cap, tok), jnp.float32)
        for route in range(top):
            local = route_ref[route : route + 1, :] - first_slot
            hit = hit + jnp.where(slot == local, 1.0, 0.0)
        rows = jnp.dot(
            hit.astype(jnp.bfloat16), source_ref[:, columns(chunk)],
            preferred_element_type=jnp.float32,
        )
        packed[kind, :, :, columns(chunk)] = rows.astype(jnp.bfloat16).reshape(half, cap, part)
        others(lambda step: outgoing(kind, step, chunk).start())
        arrived[kind, mine, :, columns(chunk)] = packed[kind, seat, :, columns(chunk)]

    def forward(kind, send_back):
        def group(index, carry):
            first = index * per

            sent, received = send_sem.at[kind], recv_sem.at[kind, index]

            @pl.when(first == mine)
            def _():
                dummy(arrived.at[kind, pl.ds(first + 1, per - 1)], sent, received).wait_recv()

            @pl.when(first != mine)
            def _():
                dummy(arrived.at[kind, pl.ds(first, per)], sent, received).wait_recv()

            rows = arrived[kind, pl.ds(first, per)].reshape(per * cap, width)
            gate = jnp.dot(rows, gate_buf[...], preferred_element_type=jnp.float32)
            upper = jnp.dot(rows, up_buf[...], preferred_element_type=jnp.float32)
            hidden = (gate / (1.0 + jnp.exp(-gate)) * upper).astype(jnp.bfloat16)
            for chunk in range(CHUNKS):
                product = jnp.dot(
                    hidden, down_buf[:, columns(chunk)], preferred_element_type=jnp.float32
                )
                result[kind, pl.ds(first, per), :, columns(chunk)] = product.astype(
                    jnp.bfloat16
                ).reshape(per, cap, part)
                if send_back:
                    others(lambda step: backward(kind, step, chunk).start(), first, first + per)
            return carry

        lax.fori_loop(0, half // per, group, 0)
        returned[kind, seat] = result[kind, mine]

    row = lax.broadcasted_iota(jnp.int32, (tok, tok), 0)
    col = lax.broadcasted_iota(jnp.int32, (tok, tok), 1)

    def upright(line):
        return jnp.sum(jnp.where(row == col, line, 0.0), axis=1, keepdims=True)

    def choices(route_ref):
        slot = lax.broadcasted_iota(jnp.int32, (tok, half * cap), 1).astype(jnp.float32)
        picks = []
        for route in range(top):
            local = upright(route_ref[route : route + 1, :]) - first_slot
            pick = jnp.where(slot == local, 1.0, 0.0).astype(jnp.bfloat16)
            picks.append((pick, upright(route_ref[top + route : top + route + 1, :])))
        return picks

    def combine(kind, picks, chunk):
        view = returned.at[kind, pl.ds(0, half - 1), :, columns(chunk)]
        dummy(view, back_send.at[kind], back_recv.at[kind, chunk]).wait_recv()
        block = returned[kind, :, :, columns(chunk)].reshape(half * cap, part)
        total = None
        for pick, weight in picks:
            term = weight * jnp.dot(pick, block, preferred_element_type=jnp.float32)
            total = term if total is None else total + term
        return total

    info_copy.start()
    for copy in row_copies:
        copy.start()
    for chunk in range(CHUNKS):
        dispatch(0, normed_ref, info_ref, chunk)
    info_copy.wait_recv()
    for chunk in range(CHUNKS):
        row_copies[chunk].wait_recv()
        dispatch(1, far_rows, far_info, chunk)
    for load in weight_loads:
        load.wait()
    forward(0, False)
    forward(1, True)
    for chunk in range(CHUNKS):
        others(lambda step: backward(0, step, chunk).start())
    far_picks = choices(far_info)
    for chunk in range(CHUNKS):
        partial[chunk] = combine(1, far_picks, chunk).astype(jnp.bfloat16)
        sum_copy(chunk).start()
    picks = choices(info_ref)
    for chunk in range(CHUNKS):
        total = combine(0, picks, chunk)
        sum_copy(chunk).wait_recv()
        total = total + incoming[chunk].astype(jnp.float32)
        total = total + mid_ref[:, columns(chunk)].astype(jnp.float32)
        out_ref[:, columns(chunk)] = total.astype(jnp.bfloat16)

    info_copy.wait_send()
    for chunk in range(CHUNKS):
        row_copies[chunk].wait_send()
        sum_copy(chunk).wait_send()

    for kind in range(2):
        whole = pl.ds(0, half - 1)
        dummy(packed.at[kind, whole], send_sem.at[kind], recv_sem.at[kind, 0]).wait_send()
        dummy(result.at[kind, whole], back_send.at[kind], back_recv.at[kind, 0]).wait_send()


def layer_kernel(sp_size, dp_size, head_size, per, top, *refs):
    inputs, out_ref, scratch = refs[:15], refs[15], refs[16:]
    (
        q_ref, k_ref, v_ref, weight_ref, resid_ref, gate_ref, up_ref, down_ref,
    ) = inputs[:8]
    small = scratch[:7]
    gate_buf, up_buf, down_buf, mid_ref, normed_ref, info_ref = scratch[7:13]
    small_sem, load_sem = scratch[13:15]
    attention_scratch, expert_scratch = scratch[15:38], scratch[38:-5]
    q_raw, k_raw, q_src, k_src, stage_sem = scratch[-5:]
    stage_loads = [
        pltpu.make_async_copy(source, target, stage_sem.at[index])
        for index, (source, target) in enumerate(((q_ref, q_raw), (k_ref, k_raw)))
    ]
    small_loads = [
        pltpu.make_async_copy(source, target, small_sem.at[index])
        for index, (source, target) in enumerate(zip(inputs[8:], small))
    ]
    weight_loads = [
        pltpu.make_async_copy(source, target, load_sem.at[index])
        for index, (source, target) in enumerate(
            ((gate_ref, gate_buf), (up_ref, up_buf), (down_ref, down_buf))
        )
    ]
    for load in stage_loads + small_loads:
        load.start()
    n = sp_size * dp_size
    me = lax.axis_index("sp") * dp_size + lax.axis_index("dp")
    barrier = pltpu.get_barrier_semaphore()

    def greet(step, carry):
        other = (me + step) % n
        pl.semaphore_signal(
            barrier, inc=1, device_id={"sp": other // dp_size, "dp": other % dp_size},
            device_id_type=MESH,
        )
        return carry

    lax.fori_loop(1, n, greet, 0)
    for load in stage_loads + small_loads:
        load.wait()
    q_gain = jnp.concatenate([small[1][...]] * (LANES // head_size), axis=1)
    k_gain = jnp.concatenate([small[2][...]] * (LANES // head_size), axis=1)

    def norm_columns(block, carry):
        here = place(block, LANES)
        for raw, normed, gain, scale in (
            (q_raw, q_src, q_gain, head_size ** (-0.5)), (k_raw, k_src, k_gain, 1.0),
        ):
            floats = raw[:, here].astype(jnp.float32)
            floats = floats * lax.rsqrt(half_means(floats * floats, head_size) + EPS)
            rounded = (floats * gain).astype(jnp.bfloat16)
            if scale != 1.0:
                rounded = (rounded.astype(jnp.float32) * scale).astype(jnp.bfloat16)
            normed[:, here] = rounded
        return carry

    lax.fori_loop(0, q_raw.shape[1] // LANES, norm_columns, 0)
    pl.semaphore_wait(barrier, n - 1)
    attention_stage(
        sp_size, dp_size, head_size, weight_loads,
        q_src, k_src, v_ref, weight_ref, resid_ref, *small,
        mid_ref, normed_ref, info_ref, *attention_scratch,
    )
    expert_stage(
        sp_size, dp_size, per, top, weight_loads,
        mid_ref, normed_ref, info_ref, gate_buf, up_buf, down_buf, out_ref, *expert_scratch,
    )


def run_layer(
    queries, keys, values, out_weight, resid, gate, upper, down,
    decay, query_gain, key_gain, norm_gain, routes, group_weight, inner_share,
):
    tok, width = queries.shape
    sp_size, dp_size = lax.axis_size("sp"), lax.axis_size("dp")
    top = routes.shape[0]
    head_size = query_gain.shape[1]
    inner = LANES // head_size
    pairs = width // sp_size // LANES
    length = sp_size * tok
    n = sp_size * dp_size
    half = n // 2
    cap = 2 * tok * top // n
    per = max(1, min(half // 2, LANES // cap))
    small = (decay, query_gain, key_gain, norm_gain, routes, group_weight, inner_share)
    dma = pltpu.SemaphoreType.DMA
    rows = pltpu.VMEM((tok, width), jnp.bfloat16)
    info = pltpu.VMEM((INFO_ROWS, tok), jnp.float32)
    head_pairs = pltpu.VMEM((pairs, length, LANES), jnp.bfloat16)
    blocks = pltpu.VMEM((2, half, cap, width), jnp.bfloat16)
    sums = pltpu.VMEM((CHUNKS, tok, width // CHUNKS), jnp.bfloat16)
    chunk_flags = dma((CHUNKS,))
    scratch = [pltpu.VMEM(array.shape, array.dtype) for array in small]
    scratch += [pltpu.VMEM(array.shape, array.dtype) for array in (gate, upper, down)]
    scratch += [rows, rows, info, dma((len(small),)), dma((3,))]
    attention_scratch = [
        rows,
        pltpu.VMEM((dp_size,) + out_weight.shape, jnp.bfloat16),
        rows,
        head_pairs,
        head_pairs,
        head_pairs,
        pltpu.VMEM((inner, length, LANES), jnp.bfloat16),
        pltpu.VMEM((length, 2 * LANES), jnp.bfloat16),
        head_pairs,
        dma((3, pairs)),
        dma((3,)),
        dma((3, pairs)),
        dma((pairs,)),
        dma,
        dma,
        dma,
        dma((2, dp_size // 2)),
        dma((2, dp_size // 2)),
        dma((dp_size // 2,)),
        dma((dp_size // 2,)),
        dma,
        dma((dp_size // 2, sp_size // DEPTH)),
        dma((dp_size // 2, sp_size // DEPTH)),
    ]
    expert_scratch = [
        rows, info, blocks, blocks, blocks, blocks, sums, sums,
        dma((2,)), chunk_flags, chunk_flags,
        dma((2,)), dma((2, half // per)), dma((2,)), dma((2, CHUNKS)),
        chunk_flags, chunk_flags,
        rows, rows, rows, rows, dma((2,)),
    ]
    in_hbm = pl.BlockSpec(memory_space=pltpu.HBM)
    return pl.pallas_call(
        functools.partial(layer_kernel, sp_size, dp_size, head_size, per, top),
        out_shape=jax.ShapeDtypeStruct((tok, width), jnp.bfloat16),
        in_specs=[in_hbm] * 15,
        out_specs=pl.BlockSpec(memory_space=pltpu.VMEM),
        scratch_shapes=scratch + attention_scratch + expert_scratch,
        compiler_params=pltpu.CompilerParams(
            collective_id=0, has_side_effects=True, vmem_limit_bytes=VMEM_LIMIT
        ),
        name="layer",
    )(queries, keys, values, out_weight, resid, gate, upper, down, *small)


VMEM_LIMIT = 62 * 1024 * 1024


def shards(
    resid,
    queries,
    keys,
    values,
    forget_cache,
    query_gain,
    key_gain,
    out_weight,
    norm_gain,
    routes,
    group_weight,
    inner_share,
    expert_gate,
    expert_up,
    expert_down,
):
    total = run_layer(
        queries[0], keys[0], values[0], out_weight, resid[0],
        expert_gate[0], expert_up[0], expert_down[0],
        forget_cache[0], query_gain[None], key_gain[None], norm_gain[None],
        routes[0].T, group_weight, inner_share[0].T,
    )
    return total[None]


def solution(mesh):
    return jax.shard_map(
        shards,
        mesh=mesh,
        in_specs=(
            P("dp", "sp", None),
            P("dp", "sp", None),
            P("dp", "sp", None),
            P("dp", "sp", None),
            P("dp", "sp", None),
            P(),
            P(),
            P(None, "dp"),
            P(),
            P("dp", "sp", None),
            P("dp", "sp"),
            P("dp", "sp", None),
            P(("sp", "dp"), None, None),
            P(("sp", "dp"), None, None),
            P(("sp", "dp"), None, None),
        ),
        out_specs=P("dp", "sp", None),
        check_vma=False,
    )
```

```python
import functools

import jax
import jax.numpy as jnp
from jax import lax
from jax.experimental import pallas as pl
from jax.experimental.pallas import tpu as pltpu
from jax.sharding import PartitionSpec as P

EPS = 1e-06


MESH = pl.DeviceIdType.MESH
LANES = 128
BLOCK = 256
DEPTH = 4


def place(index, size):
    return pl.ds(pl.multiple_of(index * size, size), size)


def half_means(squares, head_size):
    lane = lax.broadcasted_iota(jnp.int32, (LANES, LANES), 0) // head_size
    other = lax.broadcasted_iota(jnp.int32, (LANES, LANES), 1) // head_size
    same = (lane == other).astype(jnp.float32).astype(jnp.bfloat16)
    high = squares.astype(jnp.bfloat16)
    low = (squares - high.astype(jnp.float32)).astype(jnp.bfloat16)
    total = jnp.dot(high, same, preferred_element_type=jnp.float32)
    total = total + jnp.dot(low, same, preferred_element_type=jnp.float32)
    return total * (1.0 / head_size)


def far_row_copy(normed_ref, far_rows, row_send, row_recv, columns, chunk):
    half_line = lax.axis_size("sp") // 2
    line = lax.rem(lax.axis_index("sp") + half_line, 2 * half_line)
    return pltpu.make_async_remote_copy(
        src_ref=normed_ref.at[:, columns],
        dst_ref=far_rows.at[:, columns],
        send_sem=row_send.at[chunk],
        recv_sem=row_recv.at[chunk],
        device_id={"sp": line},
        device_id_type=MESH,
    )


def far_info_copy(info_ref, far_info, info_sem):
    half_line = lax.axis_size("sp") // 2
    line = lax.rem(lax.axis_index("sp") + half_line, 2 * half_line)
    return pltpu.make_async_remote_copy(
        src_ref=info_ref, dst_ref=far_info, send_sem=info_sem.at[0], recv_sem=info_sem.at[1],
        device_id={"sp": line}, device_id_type=MESH,
    )


def attention_stage(
    n, dp_size, head_size, weight_loads, send_rows,
    q_ref, k_ref, v_ref, weight_ref, resid_ref,
    decay_ref, q_gain_ref, k_gain_ref, norm_gain_ref, routes_ref, group_ref, share_ref,
    mid_ref, normed_ref, info_ref, out_ref, weights, resid_buf,
    q_buf, k_buf, v_buf, k_head, v_ones, o_buf,
    local_sem, send_sem, recv_sem, own_sem, back_send, back_recv,
    weight_sem, weight_send, weight_recv, pass_send, pass_recv, resid_sem,
    spread_send, spread_recv,
):
    me = lax.axis_index("sp")
    column = lax.axis_index("dp")
    rows_y = dp_size // 2
    row_y, core = column // 2, column % 2
    twin = row_y * 2 + 1 - core
    tok = q_ref.shape[0]
    pairs, length = q_buf.shape[0], q_buf.shape[1]
    inner = LANES // head_size
    sources, buffers = (q_ref, k_ref, v_ref), (q_buf, k_buf, v_buf)

    width_x = n // DEPTH
    x, plane_x = me % width_x, me - me % width_x
    rows = weight_ref.shape[0]
    share = rows // 2 // width_x

    def weight_rows(part):
        if part is None:
            return pl.ds(0, rows // 2)
        return pl.ds(pl.multiple_of(rows // 2 + part * share, share), share)

    def weight_block(step):
        return lax.rem(row_y + rows_y - step, rows_y) * 2 + core

    def weight_across(step, part, kind):
        return pltpu.make_async_remote_copy(
            src_ref=weight_ref.at[weight_rows(part), :],
            dst_ref=weights.at[column, weight_rows(part), :],
            send_sem=weight_send.at[kind, step],
            recv_sem=weight_recv.at[kind, step],
            device_id={"dp": lax.rem(row_y + step, rows_y) * 2 + core},
            device_id_type=MESH,
        )

    def weight_spread(step, turn, part):
        piece = weights.at[weight_block(step), weight_rows(part), :]
        return pltpu.make_async_remote_copy(
            src_ref=piece,
            dst_ref=piece,
            send_sem=spread_send.at[step, turn],
            recv_sem=spread_recv.at[step, turn],
            device_id={"sp": plane_x + lax.rem(x + turn, width_x)},
            device_id_type=MESH,
        )

    def weight_pass(step):
        block = weight_block(step)
        return pltpu.make_async_remote_copy(
            src_ref=weight_ref if step == 0 else weights.at[block],
            dst_ref=weights.at[block],
            send_sem=pass_send.at[step],
            recv_sem=pass_recv.at[step],
            device_id={"dp": twin},
            device_id_type=MESH,
        )

    weight_own = pltpu.make_async_copy(weight_ref, weights.at[column], weight_sem)

    def outgoing(kind, pair, step):
        target = lax.rem(me + step, n)
        return pltpu.make_async_remote_copy(
            src_ref=sources[kind].at[:, place(target * pairs + pair, LANES)],
            dst_ref=buffers[kind].at[pair, place(me, tok), :],
            send_sem=send_sem.at[kind],
            recv_sem=recv_sem.at[kind, pair],
            device_id={"sp": target},
            device_id_type=MESH,
        )

    def every_outgoing(kind, pair):
        view = buffers[kind].at[pair, pl.ds(0, (n - 1) * tok), :]
        return pltpu.make_async_remote_copy(
            src_ref=view, dst_ref=view, send_sem=send_sem.at[kind],
            recv_sem=recv_sem.at[kind, pair], device_id={"dp": twin}, device_id_type=MESH,
        )

    def own(kind, pair):
        return pltpu.make_async_copy(
            sources[kind].at[:, place(me * pairs + pair, LANES)],
            buffers[kind].at[pair, place(me, tok), :],
            local_sem.at[kind, pair],
        )

    def backward(pair, target):
        return pltpu.make_async_remote_copy(
            src_ref=o_buf.at[pair, pl.ds(target * tok, tok), :],
            dst_ref=out_ref.at[:, place(me * pairs + pair, LANES)],
            send_sem=back_send,
            recv_sem=back_recv,
            device_id={"sp": target},
            device_id_type=MESH,
        )

    def own_back(pair):
        return pltpu.make_async_copy(
            o_buf.at[pair, place(me, tok), :],
            out_ref.at[:, place(me * pairs + pair, LANES)],
            own_sem.at[pair],
        )

    for pair in range(pairs):
        for step in range(1, n):
            for kind in range(3):
                outgoing(kind, pair, step).start()
        for kind in range(3):
            own(kind, pair).start()

    for step in range(1, rows_y):
        weight_across(step, x, 0).start()
    for step in range(1, rows_y):
        weight_across(step, None, 1).start()
    weight_pass(0).start()
    weight_own.start()
    load_resid = pltpu.make_async_copy(resid_ref, resid_buf, resid_sem)
    load_resid.start()
    for load in weight_loads:
        load.start()
    info_ref[...] = routing_info(routes_ref, group_ref, share_ref, n * dp_size)
    send_rows(0)
    row = lax.broadcasted_iota(jnp.int32, (BLOCK, BLOCK), 0)
    col = lax.broadcasted_iota(jnp.int32, (BLOCK, BLOCK), 1)
    lane = lax.broadcasted_iota(jnp.int32, (length, LANES), 1) // head_size
    out_lane = lax.broadcasted_iota(jnp.int32, (BLOCK, LANES), 1) // head_size
    v_ones[:, LANES:] = jnp.ones((length, LANES), jnp.bfloat16)

    def scores_of(queries, keys):
        return lax.dot_general(
            queries, keys, (((1,), (1,)), ((), ())), preferred_element_type=jnp.float32
        )

    def one_pair(pair, carry):
        for kind in range(3):
            own(kind, pair).wait()
            every_outgoing(kind, pair).wait_recv()
        floats = k_buf[pair].astype(jnp.float32)
        for head in range(inner):
            k_head[head] = jnp.where(lane == head, floats, 0.0).astype(jnp.bfloat16)
        v_ones[:, :LANES] = v_buf[pair]
        for block in range(length // BLOCK):
            first = block * BLOCK
            here = slice(first, first + BLOCK)
            query_block = q_buf[pair, here, :]
            merged = None
            for head in range(inner):
                decay = decay_ref[pl.ds(pair * inner + head, 1), :]
                decay_here = decay[:, here]
                query_decay = jnp.sum(
                    jnp.where(row == col, decay_here, 0.0), axis=1, keepdims=True
                )
                near = scores_of(query_block, k_head[head, here, :])
                near = near + (query_decay - decay_here)
                near = jnp.where(col <= row, near, -jnp.inf)
                highest = jnp.max(near, axis=1, keepdims=True)
                if block > 0:
                    far = scores_of(query_block, k_head[head, :first, :])
                    far = far + (query_decay - decay[:, :first])
                    highest = jnp.maximum(highest, jnp.max(far, axis=1, keepdims=True))
                total = jnp.dot(
                    jnp.exp(near - highest).astype(jnp.bfloat16),
                    v_ones[here, :],
                    preferred_element_type=jnp.float32,
                )
                if block > 0:
                    total = total + jnp.dot(
                        jnp.exp(far - highest).astype(jnp.bfloat16),
                        v_ones[:first, :],
                        preferred_element_type=jnp.float32,
                    )
                result = total[:, :LANES] / total[:, LANES:]
                merged = result if head == 0 else jnp.where(out_lane == head, result, merged)
            o_buf[pair, here, :] = merged.astype(jnp.bfloat16)
            for target in range(first // tok, (first + BLOCK) // tok):
                @pl.when(target == me)
                def _():
                    own_back(pair).start()

                @pl.when(target != me)
                def _():
                    backward(pair, target).start()

        @pl.when(pair == 0)
        def _():
            for step in range(1, rows_y):
                weight_across(step, x, 0).wait_recv()
                for turn in range(1, width_x):
                    weight_spread(step, turn, x).start()

        return carry

    lax.fori_loop(0, pairs, one_pair, 0)
    for step in range(1, rows_y):
        weight_across(step, None, 1).wait_recv()
        for turn in range(1, width_x):
            weight_spread(step, turn, lax.rem(x + width_x - turn, width_x)).wait_recv()
        weight_pass(step).start()

    def finish(pair, carry):
        own_back(pair).wait()
        for kind in range(3):
            every_outgoing(kind, pair).wait_send()
        return carry

    lax.fori_loop(0, pairs, finish, 0)
    every_back = pltpu.make_async_remote_copy(
        src_ref=o_buf.at[:, pl.ds(0, (n - 1) * tok), :],
        dst_ref=out_ref.at[:, pl.ds(0, (n - 1) * pairs * LANES)],
        send_sem=back_send, recv_sem=back_recv, device_id={"dp": twin}, device_id_type=MESH,
    )
    every_back.wait()
    weight_own.wait()
    for step in range(1, rows_y):
        weight_across(step, x, 0).wait_send()
        weight_across(step, None, 1).wait_send()
        for turn in range(1, width_x):
            weight_spread(step, turn, x).wait_send()
    for step in range(rows_y):
        weight_pass(step).wait()
    load_resid.wait()
    span = weights.shape[2]
    squares = jnp.zeros((tok, 1), jnp.float32)
    for block in range(dp_size):
        columns = slice(block * span, (block + 1) * span)
        projected = jnp.dot(
            out_ref[...], weights[block], preferred_element_type=jnp.float32
        )
        mid = (resid_buf[:, columns].astype(jnp.float32) + projected).astype(jnp.bfloat16)
        mid_ref[:, columns] = mid
        floats = mid.astype(jnp.float32)
        squares = squares + jnp.sum(floats * floats, axis=1, keepdims=True)
    factor = lax.rsqrt(squares * (1.0 / (dp_size * span)) + EPS)
    for block in range(dp_size):
        columns = slice(block * span, (block + 1) * span)
        scaled = mid_ref[:, columns].astype(jnp.float32) * factor
        normed_ref[:, columns] = (scaled * norm_gain_ref[:, columns]).astype(jnp.bfloat16)
        send_rows((block + 1) * span)


INFO_ROWS = 8


def routing_info(routes_ref, group_ref, share_ref, experts):
    top, tok = routes_ref.shape
    capacity = 2 * tok * top // experts
    expert = lax.broadcasted_iota(jnp.int32, (experts, tok), 0)
    hits = [(expert == routes_ref[r : r + 1, :]).astype(jnp.float32) for r in range(top)]
    every = sum(hits[1:], hits[0]).astype(jnp.bfloat16)
    row = lax.broadcasted_iota(jnp.int32, (tok, tok), 0)
    col = lax.broadcasted_iota(jnp.int32, (tok, tok), 1)
    before = (row < col).astype(jnp.float32).astype(jnp.bfloat16)
    earlier = jnp.dot(every, before, preferred_element_type=jnp.float32)
    shares = [share_ref[r : r + 1, :] for r in range(top)]
    total = sum(shares[1:], shares[0])
    lines = [
        routes_ref[r : r + 1, :].astype(jnp.float32) * capacity
        + jnp.sum(hits[r] * earlier, axis=0, keepdims=True)
        for r in range(top)
    ]
    lines += [group_ref[...] * shares[r] / total for r in range(top)]
    lines.append(jnp.zeros((INFO_ROWS - 2 * top, tok), jnp.float32))
    return jnp.concatenate(lines, axis=0)


CHUNKS = 4


def expert_stage(
    sp_size, dp_size, per, top, weight_loads,
    mid_ref, normed_ref, info_ref, gate_buf, up_buf, down_buf,
    out_ref,
    far_rows, far_info, packed, arrived, result, returned, partial, incoming,
    info_sem, row_send, row_recv, send_sem, recv_sem,
    back_send, back_recv, sum_send, sum_recv,
):
    n = sp_size * dp_size
    half = n // 2
    me = lax.axis_index("sp") * dp_size + lax.axis_index("dp")
    side, seat = me // half, me % half
    twin = (me + half) % n
    tok, width = normed_ref.shape
    cap = packed.shape[2]
    part = width // CHUNKS
    mine = half // 2

    def columns(chunk):
        return slice(chunk * part, (chunk + 1) * part)

    def coords(flat):
        return {"sp": lax.div(flat, dp_size), "dp": lax.rem(flat, dp_size)}

    info_copy = far_info_copy(info_ref, far_info, info_sem)
    row_copies = [
        far_row_copy(normed_ref, far_rows, row_send, row_recv, columns(chunk), chunk)
        for chunk in range(CHUNKS)
    ]

    def outgoing(kind, step, chunk):
        target = lax.rem(seat + mine + step, half)
        return pltpu.make_async_remote_copy(
            src_ref=packed.at[kind, target, :, columns(chunk)],
            dst_ref=arrived.at[kind, step, :, columns(chunk)],
            send_sem=send_sem.at[kind],
            recv_sem=recv_sem.at[kind, lax.div(step, per)],
            device_id=coords(side * half + target),
            device_id_type=MESH,
        )

    def backward(kind, step, chunk):
        target = lax.rem(seat + half + half - mine - step, half)
        return pltpu.make_async_remote_copy(
            src_ref=result.at[kind, step, :, columns(chunk)],
            dst_ref=returned.at[kind, seat, :, columns(chunk)],
            send_sem=back_send.at[kind],
            recv_sem=back_recv.at[kind, chunk],
            device_id=coords(side * half + target),
            device_id_type=MESH,
        )

    def dummy(view, sent, received):
        return pltpu.make_async_remote_copy(
            src_ref=view, dst_ref=view, send_sem=sent, recv_sem=received,
            device_id=coords(twin), device_id_type=MESH,
        )

    def sum_copy(chunk):
        return pltpu.make_async_remote_copy(
            src_ref=partial.at[chunk],
            dst_ref=incoming.at[chunk],
            send_sem=sum_send.at[chunk],
            recv_sem=sum_recv.at[chunk],
            device_id=coords(twin),
            device_id_type=MESH,
        )

    def others(action, start=0, stop=half):
        def run(step, carry):
            @pl.when(step != mine)
            def _():
                action(step)

            return carry

        lax.fori_loop(start, stop, run, 0)

    first_slot = (side * (half * cap)).astype(jnp.float32)

    def dispatch(kind, source_ref, route_ref, chunk):
        slot = lax.broadcasted_iota(jnp.int32, (half * cap, tok), 0).astype(jnp.float32)
        hit = jnp.zeros((half * cap, tok), jnp.float32)
        for route in range(top):
            local = route_ref[route : route + 1, :] - first_slot
            hit = hit + jnp.where(slot == local, 1.0, 0.0)
        rows = jnp.dot(
            hit.astype(jnp.bfloat16), source_ref[:, columns(chunk)],
            preferred_element_type=jnp.float32,
        )
        packed[kind, :, :, columns(chunk)] = rows.astype(jnp.bfloat16).reshape(half, cap, part)
        others(lambda step: outgoing(kind, step, chunk).start())
        arrived[kind, mine, :, columns(chunk)] = packed[kind, seat, :, columns(chunk)]

    def forward(kind, send_back):
        def group(index, carry):
            first = index * per

            sent, received = send_sem.at[kind], recv_sem.at[kind, index]

            @pl.when(first == mine)
            def _():
                dummy(arrived.at[kind, pl.ds(first + 1, per - 1)], sent, received).wait_recv()

            @pl.when(first != mine)
            def _():
                dummy(arrived.at[kind, pl.ds(first, per)], sent, received).wait_recv()

            rows = arrived[kind, pl.ds(first, per)].reshape(per * cap, width)
            gate = jnp.dot(rows, gate_buf[...], preferred_element_type=jnp.float32)
            upper = jnp.dot(rows, up_buf[...], preferred_element_type=jnp.float32)
            hidden = (gate / (1.0 + jnp.exp(-gate)) * upper).astype(jnp.bfloat16)
            for chunk in range(CHUNKS):
                product = jnp.dot(
                    hidden, down_buf[:, columns(chunk)], preferred_element_type=jnp.float32
                )
                result[kind, pl.ds(first, per), :, columns(chunk)] = product.astype(
                    jnp.bfloat16
                ).reshape(per, cap, part)
                if send_back:
                    others(lambda step: backward(kind, step, chunk).start(), first, first + per)
            return carry

        lax.fori_loop(0, half // per, group, 0)
        returned[kind, seat] = result[kind, mine]

    row = lax.broadcasted_iota(jnp.int32, (tok, tok), 0)
    col = lax.broadcasted_iota(jnp.int32, (tok, tok), 1)

    def upright(line):
        return jnp.sum(jnp.where(row == col, line, 0.0), axis=1, keepdims=True)

    def choices(route_ref):
        slot = lax.broadcasted_iota(jnp.int32, (tok, half * cap), 1).astype(jnp.float32)
        picks = []
        for route in range(top):
            local = upright(route_ref[route : route + 1, :]) - first_slot
            pick = jnp.where(slot == local, 1.0, 0.0).astype(jnp.bfloat16)
            picks.append((pick, upright(route_ref[top + route : top + route + 1, :])))
        return picks

    def combine(kind, picks, chunk):
        view = returned.at[kind, pl.ds(0, half - 1), :, columns(chunk)]
        dummy(view, back_send.at[kind], back_recv.at[kind, chunk]).wait_recv()
        block = returned[kind, :, :, columns(chunk)].reshape(half * cap, part)
        total = None
        for pick, weight in picks:
            term = weight * jnp.dot(pick, block, preferred_element_type=jnp.float32)
            total = term if total is None else total + term
        return total

    for chunk in range(CHUNKS):
        dispatch(0, normed_ref, info_ref, chunk)
    info_copy.wait_recv()
    for chunk in range(CHUNKS):
        row_copies[chunk].wait_recv()
        dispatch(1, far_rows, far_info, chunk)
    for load in weight_loads:
        load.wait()
    forward(0, False)
    forward(1, True)
    for chunk in range(CHUNKS):
        others(lambda step: backward(0, step, chunk).start())
    far_picks = choices(far_info)
    for chunk in range(CHUNKS):
        partial[chunk] = combine(1, far_picks, chunk).astype(jnp.bfloat16)
        sum_copy(chunk).start()
    picks = choices(info_ref)
    for chunk in range(CHUNKS):
        total = combine(0, picks, chunk)
        sum_copy(chunk).wait_recv()
        total = total + incoming[chunk].astype(jnp.float32)
        total = total + mid_ref[:, columns(chunk)].astype(jnp.float32)
        out_ref[:, columns(chunk)] = total.astype(jnp.bfloat16)

    info_copy.wait_send()
    for chunk in range(CHUNKS):
        row_copies[chunk].wait_send()
        sum_copy(chunk).wait_send()

    for kind in range(2):
        whole = pl.ds(0, half - 1)
        dummy(packed.at[kind, whole], send_sem.at[kind], recv_sem.at[kind, 0]).wait_send()
        dummy(result.at[kind, whole], back_send.at[kind], back_recv.at[kind, 0]).wait_send()


def layer_kernel(sp_size, dp_size, head_size, per, top, *refs):
    inputs, out_ref, scratch = refs[:15], refs[15], refs[16:]
    (
        q_ref, k_ref, v_ref, weight_ref, resid_ref, gate_ref, up_ref, down_ref,
    ) = inputs[:8]
    small = scratch[:7]
    gate_buf, up_buf, down_buf, mid_ref, normed_ref, info_ref = scratch[7:13]
    small_sem, load_sem = scratch[13:15]
    attention_scratch, expert_scratch = scratch[15:38], scratch[38:-5]
    q_raw, k_raw, q_src, k_src, stage_sem = scratch[-5:]
    stage_loads = [
        pltpu.make_async_copy(source, target, stage_sem.at[index])
        for index, (source, target) in enumerate(((q_ref, q_raw), (k_ref, k_raw)))
    ]
    small_loads = [
        pltpu.make_async_copy(source, target, small_sem.at[index])
        for index, (source, target) in enumerate(zip(inputs[8:], small))
    ]
    weight_loads = [
        pltpu.make_async_copy(source, target, load_sem.at[index])
        for index, (source, target) in enumerate(
            ((gate_ref, gate_buf), (up_ref, up_buf), (down_ref, down_buf))
        )
    ]
    for load in stage_loads + small_loads:
        load.start()
    n = sp_size * dp_size
    me = lax.axis_index("sp") * dp_size + lax.axis_index("dp")
    barrier = pltpu.get_barrier_semaphore()

    def greet(step, carry):
        other = (me + step) % n
        pl.semaphore_signal(
            barrier, inc=1, device_id={"sp": other // dp_size, "dp": other % dp_size},
            device_id_type=MESH,
        )
        return carry

    lax.fori_loop(1, n, greet, 0)
    for load in stage_loads + small_loads:
        load.wait()
    q_gain = jnp.concatenate([small[1][...]] * (LANES // head_size), axis=1)
    k_gain = jnp.concatenate([small[2][...]] * (LANES // head_size), axis=1)

    def norm_columns(block, carry):
        here = place(block, LANES)
        for raw, normed, gain, scale in (
            (q_raw, q_src, q_gain, head_size ** (-0.5)), (k_raw, k_src, k_gain, 1.0),
        ):
            floats = raw[:, here].astype(jnp.float32)
            floats = floats * lax.rsqrt(half_means(floats * floats, head_size) + EPS)
            rounded = (floats * gain).astype(jnp.bfloat16)
            if scale != 1.0:
                rounded = (rounded.astype(jnp.float32) * scale).astype(jnp.bfloat16)
            normed[:, here] = rounded
        return carry

    lax.fori_loop(0, q_raw.shape[1] // LANES, norm_columns, 0)
    pl.semaphore_wait(barrier, n - 1)
    far_rows, row_send, row_recv = expert_scratch[0], expert_scratch[9], expert_scratch[10]

    def send_rows(done):
        width = normed_ref.shape[1]
        part = width // CHUNKS
        if done == 0:
            far_info_copy(info_ref, expert_scratch[1], expert_scratch[8]).start()
        elif done % part == 0:
            columns, chunk = slice(done - part, done), done // part - 1
            far_row_copy(normed_ref, far_rows, row_send, row_recv, columns, chunk).start()

    attention_stage(
        sp_size, dp_size, head_size, weight_loads, send_rows,
        q_src, k_src, v_ref, weight_ref, resid_ref, *small,
        mid_ref, normed_ref, info_ref, *attention_scratch,
    )
    expert_stage(
        sp_size, dp_size, per, top, weight_loads,
        mid_ref, normed_ref, info_ref, gate_buf, up_buf, down_buf, out_ref, *expert_scratch,
    )


def run_layer(
    queries, keys, values, out_weight, resid, gate, upper, down,
    decay, query_gain, key_gain, norm_gain, routes, group_weight, inner_share,
):
    tok, width = queries.shape
    sp_size, dp_size = lax.axis_size("sp"), lax.axis_size("dp")
    top = routes.shape[0]
    head_size = query_gain.shape[1]
    inner = LANES // head_size
    pairs = width // sp_size // LANES
    length = sp_size * tok
    n = sp_size * dp_size
    half = n // 2
    cap = 2 * tok * top // n
    per = max(1, min(half // 2, LANES // cap))
    small = (decay, query_gain, key_gain, norm_gain, routes, group_weight, inner_share)
    dma = pltpu.SemaphoreType.DMA
    rows = pltpu.VMEM((tok, width), jnp.bfloat16)
    info = pltpu.VMEM((INFO_ROWS, tok), jnp.float32)
    head_pairs = pltpu.VMEM((pairs, length, LANES), jnp.bfloat16)
    blocks = pltpu.VMEM((2, half, cap, width), jnp.bfloat16)
    sums = pltpu.VMEM((CHUNKS, tok, width // CHUNKS), jnp.bfloat16)
    chunk_flags = dma((CHUNKS,))
    scratch = [pltpu.VMEM(array.shape, array.dtype) for array in small]
    scratch += [pltpu.VMEM(array.shape, array.dtype) for array in (gate, upper, down)]
    scratch += [rows, rows, info, dma((len(small),)), dma((3,))]
    attention_scratch = [
        rows,
        pltpu.VMEM((dp_size,) + out_weight.shape, jnp.bfloat16),
        rows,
        head_pairs,
        head_pairs,
        head_pairs,
        pltpu.VMEM((inner, length, LANES), jnp.bfloat16),
        pltpu.VMEM((length, 2 * LANES), jnp.bfloat16),
        head_pairs,
        dma((3, pairs)),
        dma((3,)),
        dma((3, pairs)),
        dma((pairs,)),
        dma,
        dma,
        dma,
        dma((2, dp_size // 2)),
        dma((2, dp_size // 2)),
        dma((dp_size // 2,)),
        dma((dp_size // 2,)),
        dma,
        dma((dp_size // 2, sp_size // DEPTH)),
        dma((dp_size // 2, sp_size // DEPTH)),
    ]
    expert_scratch = [
        rows, info, blocks, blocks, blocks, blocks, sums, sums,
        dma((2,)), chunk_flags, chunk_flags,
        dma((2,)), dma((2, half // per)), dma((2,)), dma((2, CHUNKS)),
        chunk_flags, chunk_flags,
        rows, rows, rows, rows, dma((2,)),
    ]
    in_hbm = pl.BlockSpec(memory_space=pltpu.HBM)
    return pl.pallas_call(
        functools.partial(layer_kernel, sp_size, dp_size, head_size, per, top),
        out_shape=jax.ShapeDtypeStruct((tok, width), jnp.bfloat16),
        in_specs=[in_hbm] * 15,
        out_specs=pl.BlockSpec(memory_space=pltpu.VMEM),
        scratch_shapes=scratch + attention_scratch + expert_scratch,
        compiler_params=pltpu.CompilerParams(
            collective_id=0, has_side_effects=True, vmem_limit_bytes=VMEM_LIMIT
        ),
        name="layer",
    )(queries, keys, values, out_weight, resid, gate, upper, down, *small)


VMEM_LIMIT = 62 * 1024 * 1024


def shards(
    resid,
    queries,
    keys,
    values,
    forget_cache,
    query_gain,
    key_gain,
    out_weight,
    norm_gain,
    routes,
    group_weight,
    inner_share,
    expert_gate,
    expert_up,
    expert_down,
):
    total = run_layer(
        queries[0], keys[0], values[0], out_weight, resid[0],
        expert_gate[0], expert_up[0], expert_down[0],
        forget_cache[0], query_gain[None], key_gain[None], norm_gain[None],
        routes[0].T, group_weight, inner_share[0].T,
    )
    return total[None]


def solution(mesh):
    return jax.shard_map(
        shards,
        mesh=mesh,
        in_specs=(
            P("dp", "sp", None),
            P("dp", "sp", None),
            P("dp", "sp", None),
            P("dp", "sp", None),
            P("dp", "sp", None),
            P(),
            P(),
            P(None, "dp"),
            P(),
            P("dp", "sp", None),
            P("dp", "sp"),
            P("dp", "sp", None),
            P(("sp", "dp"), None, None),
            P(("sp", "dp"), None, None),
            P(("sp", "dp"), None, None),
        ),
        out_specs=P("dp", "sp", None),
        check_vma=False,
    )
```
